32 devices in a mesh: sp: 8 (over z, x), tp: 4 (over y, core).
Axes of the slice: x: 2, y: 2, z: 4, core: 2. Of those that a mesh axis runs over, the one named last changes fastest.
Arguments:
- tokens_in: bfloat16 [6144, 2048], P(('sp', 'tp')), may hold values from -300 to 300
- norm_gain: float32 [2048], replicated, may hold values from 0.1 to 1.9
- query_weight: bfloat16 [2048, 1024], P('sp', 'tp'), may hold values from -64 to 64
- key_weight: bfloat16 [2048, 512], P('sp', 'tp'), may hold values from -1 to 1
- value_weight: bfloat16 [2048, 512], P('sp', 'tp'), may hold values from -0.125 to 0.125
- pool_weight: bfloat16 [2048, 1024], P('sp', 'tp'), may hold values from -0.125 to 0.125
- sink_logit: float32 [16], P('tp'), may hold values from 1 to 5
- pool_gain: float32 [1024], P('tp'), may hold values from 0.1 to 1.9
- attention_out_weight: bfloat16 [1024, 2048], P('tp', 'sp'), may hold values from -0.125 to 0.125
- pool_out_weight: bfloat16 [1024, 2048], P('tp', 'sp'), may hold values from -0.1875 to 0.1875
Outputs:
- mixed_out: bfloat16 [6144, 2048], P(('sp', 'tp'))
The draws below stay inside these ranges and needn't reach their ends.
All inputs are finite; a program needn't handle non-finite values.
Results may differ from the reference program's by a relative error of at most 0.014.
Values may be sent and summed in bfloat16 or wider, within the bound.
A program may use at most 64 MiB of HBM per device.

```python
import jax
import jax.numpy as jnp
from jax import lax

D = 2048
HEADS = 16
KV_HEADS = 8
HEAD_DIM = 64
POOL_CH = 256
POOL_GROUPS = 4
WINDOW = 128
TOK_DEV = 768
TOKENS = 6144
Q_WIDTH = 1024
KV_WIDTH = 512
POOL_WIDTH = 1024
N_TP = 4


def draw_tokens_in(key, part):
    noise_key = jax.random.fold_in(key, 11)
    direction_key = jax.random.fold_in(key, 12)
    level_key = jax.random.fold_in(key, 13)
    rough = jax.random.normal(noise_key, (TOKENS, D), jnp.float32)
    direction = jax.random.normal(direction_key, (D,), jnp.float32)
    block_count = TOKENS // TOK_DEV
    block_number = jnp.arange(block_count)
    ramp = block_number.astype(jnp.float32) / max(block_count - 1, 1)
    alternate = (1 - 2 * (block_number % 2)).astype(jnp.float32)
    jitter = jax.random.uniform(level_key, (block_count,), jnp.float32, 0.8, 1.3)
    levels = 2.0 * 3.0 ** ramp * jitter * alternate
    level_rows = jnp.repeat(levels, TOK_DEV)
    values = rough + level_rows[:, None] * direction[None, :]
    return jnp.clip(values, -300.0, 300.0).astype(jnp.bfloat16)


def key_base(key):
    limit = 6.0 * D ** (-0.5)
    base = jax.random.normal(jax.random.fold_in(key, 71), (D, KV_HEADS * HEAD_DIM), jnp.float32) * D ** (-0.5)
    base = jnp.clip(base, -limit, limit)
    return base


def draw_key_weight(key, part):
    return jnp.clip(key_base(key), -1.0, 1.0).astype(jnp.bfloat16)


def draw_query_weight(key, part):
    limit = 6.0 * D ** (-0.5)
    own = jax.random.normal(jax.random.fold_in(key, 72), (D, HEADS * HEAD_DIM), jnp.float32) * D ** (-0.5)
    own = jnp.clip(own, -limit, limit)
    return jnp.clip(own, -64.0, 64.0).astype(jnp.bfloat16)


def with_spikes(values, key, source, target, blocks, factor):
    owner, partner = [(jnp.arange(values.shape[dim]) // (values.shape[dim] // blocks)).reshape([-1 if axis == dim else 1 for axis in range(values.ndim)]) for dim in (source, target)]
    chosen = jax.random.permutation(key, blocks)[partner]
    strong = (owner == chosen) | (owner == (partner + blocks // 2) % blocks)
    return jnp.where(strong, factor * values, values)


def level_of(key, shape, split, low, largest):
    level = 1.0
    for dim, shards_of in split:
        steps = jax.random.uniform(jax.random.fold_in(jax.random.fold_in(key, 6), dim), (shards_of,), jnp.float32, low / len(split), largest / len(split))
        level = level * jnp.repeat(jnp.exp(steps), shape[dim] // shards_of).reshape((-1,) + (1,) * (len(shape) - 1 - dim))
    return level


def bell_draw(stream_key, dims, deviation, most, pieces=(), held_as=jnp.bfloat16):
    drawn = deviation * jax.random.normal(stream_key, dims, jnp.float32)
    if pieces:
        drawn = drawn * level_of(stream_key, dims, pieces, -0.22, 0.18)
    return jnp.clip(drawn, -most, most).astype(held_as)


def bell_draw_with(rng, dims, deviation, bound, shards, heavy, dtype=jnp.bfloat16):
    drawn = deviation * jax.random.normal(rng, dims, jnp.float32)
    if shards:
        drawn = drawn * level_of(rng, dims, shards, -0.22, 0.18)
    return jnp.clip(with_spikes(drawn, jax.random.fold_in(rng, 3), *heavy), -bound, bound).astype(dtype)


def setup_inputs(seed: int = 0) -> dict:
    keys = jax.random.split(jax.random.key(seed), 11)
    return {
        "tokens_in": draw_tokens_in(jax.random.fold_in(keys[10], 71), 0),
        "norm_gain": jnp.clip(1.0 + 0.18 * jax.random.normal(keys[1], (D,), jnp.float32), 0.1, 1.9),
        "query_weight": draw_query_weight(jax.random.fold_in(keys[10], 71), 0),
        "key_weight": draw_key_weight(jax.random.fold_in(keys[10], 71), 0),
        "value_weight": bell_draw(keys[4], (D, KV_WIDTH), D ** -0.5, 0.125, ((0, 8), (1, 4))),
        "pool_weight": bell_draw(keys[5], (D, POOL_WIDTH), D ** -0.5, 0.125, ((0, 8), (1, 4))),
        "sink_logit": jnp.clip(1.0 + 4.0 * jax.random.uniform(keys[6], (HEADS,), jnp.float32) ** level_of(keys[6], (HEADS,), ((0, 4),), -0.2, 0.2), 1.0, 5.0),
        "pool_gain": jnp.clip(1.0 + 0.18 * jax.random.normal(keys[7], (POOL_WIDTH,), jnp.float32), 0.1, 1.9),
        "attention_out_weight": bell_draw(keys[8], (Q_WIDTH, D), (Q_WIDTH + POOL_WIDTH) ** -0.5, 0.125, ((0, 4), (1, 8))),
        "pool_out_weight": bell_draw_with(keys[9], (POOL_WIDTH, D), (Q_WIDTH + POOL_WIDTH) ** -0.5, 0.1875, ((0, 4), (1, 8)), (0, 1, 8, 2.0)),
    }


EPS = 1e-06
SHORT_REACHES = (8, 32)

def attention_mix(query_rows, key_rows, value_rows, sink_logit):
    total_rows = query_rows.shape[0]
    blocks = total_rows // WINDOW
    group = HEADS // KV_HEADS
    queries = query_rows.astype(jnp.float32).reshape(blocks, WINDOW, KV_HEADS, group, HEAD_DIM)
    key_blocks = key_rows.astype(jnp.float32).reshape(blocks, WINDOW, KV_HEADS, HEAD_DIM)
    value_blocks = value_rows.astype(jnp.float32).reshape(blocks, WINDOW, KV_HEADS, HEAD_DIM)

    def with_previous(blocks_in):
        earlier = jnp.concatenate([jnp.zeros_like(blocks_in[:1]), blocks_in[:-1]], axis=0)
        return jnp.concatenate([earlier, blocks_in], axis=1)
    key_pairs = with_previous(key_blocks)
    value_pairs = with_previous(value_blocks)
    scores = jnp.einsum('nqhgd,nkhd->nhgqk', queries, key_pairs) * HEAD_DIM ** (-0.5)
    q_index = jnp.arange(WINDOW)[:, None]
    k_index = jnp.arange(2 * WINDOW)[None, :]
    distance = q_index + WINDOW - k_index
    inside = (distance >= 0) & (distance < WINDOW)
    block_index = jnp.arange(blocks)[:, None, None]
    allowed = inside[None] & ((block_index > 0) | (k_index >= WINDOW)[None])
    scores = jnp.where(allowed[:, None, None], scores, -jnp.inf)
    sinks = sink_logit.astype(jnp.float32).reshape(1, KV_HEADS, group, 1, 1)
    peak = jnp.maximum(lax.optimization_barrier(jnp.max(scores, axis=-1, keepdims=True)), sinks)
    expo = jnp.exp(scores - peak)
    denom = lax.optimization_barrier(jnp.sum(expo, axis=-1, keepdims=True)) + jnp.exp(sinks - peak)
    probs = lax.optimization_barrier((expo / denom).astype(jnp.bfloat16))
    attended = jnp.einsum('nhgqk,nkhd->nqhgd', probs.astype(jnp.float32), value_pairs)
    return attended.astype(jnp.bfloat16).reshape(total_rows, HEADS * HEAD_DIM)

def pool_mix(pool_rows, pool_gain):
    total_rows = pool_rows.shape[0]
    values = pool_rows.astype(jnp.float32)
    running = jnp.concatenate([jnp.zeros((1, values.shape[1]), jnp.float32), jnp.cumsum(values, axis=0)], axis=0)
    position = jnp.arange(total_rows)
    outputs = []
    for group_index, reach in enumerate(SHORT_REACHES + (WINDOW,)):
        span = running[:, group_index * POOL_CH:(group_index + 1) * POOL_CH]
        lower = span[jnp.maximum(position + 1 - reach, 0)]
        count = jnp.minimum(position + 1, reach).astype(jnp.float32)[:, None]
        outputs.append((span[1:] - lower) / count)
    whole_prefix = running[1:, (POOL_GROUPS - 1) * POOL_CH:] / (position + 1).astype(jnp.float32)[:, None]
    pooled = jnp.concatenate(outputs + [whole_prefix], axis=1)
    return ((pooled - values) * pool_gain.astype(jnp.float32)).astype(jnp.bfloat16)

def reference(tokens_in, norm_gain, query_weight, key_weight, value_weight, pool_weight, sink_logit, pool_gain, attention_out_weight, pool_out_weight):
    widened = tokens_in.astype(jnp.float32)
    inverse = lax.rsqrt(lax.optimization_barrier(jnp.mean(widened * widened, axis=1, keepdims=True)) + EPS)
    normed = (widened * inverse * norm_gain.astype(jnp.float32)).astype(jnp.bfloat16)
    query_rows = jnp.dot(normed, query_weight, preferred_element_type=jnp.float32).astype(jnp.bfloat16)
    key_rows = jnp.dot(normed, key_weight, preferred_element_type=jnp.float32).astype(jnp.bfloat16)
    value_rows = jnp.dot(normed, value_weight, preferred_element_type=jnp.float32).astype(jnp.bfloat16)
    pool_rows = jnp.dot(normed, pool_weight, preferred_element_type=jnp.float32).astype(jnp.bfloat16)
    attended = attention_mix(query_rows, key_rows, value_rows, sink_logit)
    pool_mixed = pool_mix(pool_rows, pool_gain)
    attend_cols = Q_WIDTH // N_TP
    pool_cols = POOL_WIDTH // N_TP
    summed = jnp.zeros((tokens_in.shape[0], D), jnp.float32)
    for block in range(N_TP):
        partial_sum = jnp.dot(attended[:, block * attend_cols:(block + 1) * attend_cols], attention_out_weight[block * attend_cols:(block + 1) * attend_cols], preferred_element_type=jnp.float32)
        partial_sum = partial_sum + jnp.dot(pool_mixed[:, block * pool_cols:(block + 1) * pool_cols], pool_out_weight[block * pool_cols:(block + 1) * pool_cols], preferred_element_type=jnp.float32)
        rounded = lax.optimization_barrier(partial_sum.astype(jnp.bfloat16))
        summed = summed + rounded.astype(jnp.float32)
    return summed.astype(jnp.bfloat16)
```

```python
import functools
import math

import jax
import jax.numpy as jnp
from jax import lax
from jax.experimental import pallas as pl
from jax.experimental.pallas import tpu as pltpu
from jax.sharding import PartitionSpec as P

HEAD_DIM = 64
POOL_CH = 256
POOL_GROUPS = 4
WINDOW = 128
EPS = 1e-06
SHORT_REACHES = (8, 32)
CORES = 2
SEND_SLOTS = 32
MESH = pl.DeviceIdType.MESH
F32 = jnp.float32
BF16 = jnp.bfloat16


def when(cond, fn):
    if cond is None:
        fn()
    else:
        pl.when(cond)(fn)


def both(a, b):
    return b if a is None else (a if b is None else jnp.logical_and(a, b))


def kernel(n_sp, n_tp, cols, n_in, n_out, widths, *refs):
    tok, gain, sink, pgain = refs[:4]
    win_refs = refs[4 : 4 + n_in]
    wout_refs = refs[4 + n_in : 4 + n_in + n_out]
    (
        out, tokv, xs, wq, wkv, wp, wa, wb, acc, ext, mix, tot, carry, dfar, rfar, dnear, rnear,
        ysend, yrecv, ofar, onear,
        local_sem, send_sem, sem_q, sem_kv, sem_p, sem_a, sem_b, sem_b_side,
        sem_tok, sem_halo, sem_tot, sem_far, sem_near, sem_y,
    ) = refs[4 + n_in + n_out :]
    qw, kw, vw, pw = widths
    levels = n_sp // cols
    chips = n_tp // CORES
    rows, seq = tok.shape[0], xs.shape[1]
    per = rows * CORES
    channel0 = qw + kw + vw
    blocks = seq // WINDOW
    me, t = lax.axis_index("sp"), lax.axis_index("tp")
    z, x = me // cols, me % cols
    y, c = t // CORES, t % CORES
    partner = y * CORES + (1 - c)
    up, down = z + 1 < levels, z > 0
    later, earlier = me + 1 < n_sp, me > 0

    locals_ = []

    def fetch(src, dst):
        copy = pltpu.make_async_copy(src, dst, local_sem.at[len(locals_)])
        copy.start()
        locals_.append(copy)

    fetch(win_refs[0], wq.at[me])
    at = 0
    for ref in win_refs[1:-1]:
        w = ref.shape[1]
        fetch(ref, wkv.at[me, :, pl.ds(at, w)])
        at += w
    fetch(win_refs[-1], wp.at[me])
    fetch(tok, tokv)
    fetch(wout_refs[0], wa.at[me])
    fetch(wout_refs[1], wb.at[me])
    ext[:WINDOW, qw:] = jnp.zeros((WINDOW, ext.shape[1] - qw), BF16)

    barrier = pltpu.get_barrier_semaphore()
    next_row = jnp.logical_and(x == cols - 1, up)
    last_row = jnp.logical_and(x == 0, down)

    def greet(cond, sp, tp):
        when(
            cond,
            lambda: pl.semaphore_signal(
                barrier, inc=1, device_id=(sp, tp), device_id_type=MESH
            ),
        )

    for d in range(1, cols):
        greet(None, z * cols + (x + d) % cols, t)
    greet(up, me + cols, t)
    greet(down, me - cols, t)
    greet_diagonal = cols > 1
    if greet_diagonal:
        greet(next_row, me + 1, t)
        greet(last_row, me - 1, t)
    for d in range(1, n_tp):
        greet(None, me, (t + d) % n_tp)
    expected = cols - 1 + n_tp - 1 + jnp.where(up, 1, 0) + jnp.where(down, 1, 0)
    if greet_diagonal:
        expected = expected + jnp.where(next_row, 1, 0) + jnp.where(last_row, 1, 0)
    with jax.named_scope("barrier"):
        pl.semaphore_wait(barrier, expected)

    slots = [None] * send_sem.shape[0]
    count = [0]

    def send(cond, src, dst, recv, dev):
        slot = count[0] % len(slots)
        count[0] += 1
        if slots[slot] is not None:
            when(slots[slot][0], slots[slot][1].wait_send)
        copy = pltpu.make_async_remote_copy(
            src_ref=src, dst_ref=dst, send_sem=send_sem.at[slot], recv_sem=recv,
            device_id=dev, device_id_type=MESH,
        )
        when(cond, copy.start)
        slots[slot] = (cond, copy)

    def arrived(cond, dst, recv):
        copy = pltpu.make_async_remote_copy(
            src_ref=dst, dst_ref=dst, send_sem=send_sem.at[0], recv_sem=recv,
            device_id=(me, partner), device_id_type=MESH,
        )
        when(cond, copy.wait_recv)

    def at_distance(h):
        if h == 0:
            return ((z, None, None, None),)
        return (
            (z - h, z - h >= 0, up, me + cols),
            (z + h, z + h < levels, down, me - cols),
        )

    class Spread:
        def __init__(self, name, buf, sem, share=0.0, side_sem=None):
            self.name, self.buf, self.sem, self.side_sem = name, buf, sem, side_sem
            k = buf.shape[1]
            self.side = int(k * share) // 16 * 16 if cols > 1 and levels > 1 else 0
            self.k = k
            self.have = set()

        def piece(self, s, lo, hi):
            return self.buf.at[s] if (lo, hi) == (0, self.k) else self.buf.at[s, pl.ds(lo, hi - lo), :]

        def go(self, cond, s, lo, hi, sem, dev_sp):
            ref = self.piece(s, lo, hi)
            send(cond, ref, ref, sem.at[s], (dev_sp, t))

        def across(self, cond, s, lo=0):
            if lo == self.k:
                return
            for d in range(1, cols):
                self.go(cond, s, lo, self.k, self.sem, z * cols + (x + d) % cols)

        def begin_z(self):
            self.go(up, me, 0, self.k, self.sem, me + cols)
            self.go(down, me, 0, self.k, self.sem, me - cols)

        def begin_x(self):
            self.across(None, me)

        def forward(self, h):
            with jax.named_scope(f"f{self.name}{h}"):
                for level, there, on, to in at_distance(h):
                    s = level * cols + x
                    arrived(there, self.buf.at[s], self.sem.at[s])
                    self.go(both(there, on), s, 0, self.k, self.sem, to)
                    self.across(there, s, self.side if h == 1 else 0)

        def peers(self, level):
            return [level * cols + (x + cols - d) % cols for d in range(1, cols)]

        def forward_side(self):
            if not self.side:
                return
            self.take(0)
            sem = self.sem if self.side == self.k else self.side_sem
            for s in self.peers(z):
                self.go(up, s, 0, self.side, sem, me + cols)
                self.go(down, s, 0, self.side, sem, me - cols)

        def take(self, h):
            if h in self.have:
                return
            self.have.add(h)
            with jax.named_scope(f"t{self.name}{h}"):
                for level, there, _, _ in at_distance(h):
                    for s in self.peers(level):
                        if h == 1 and self.side and self.side < self.k:
                            arrived(there, self.piece(s, 0, self.side), self.side_sem.at[s])
                            arrived(there, self.piece(s, self.side, self.k), self.sem.at[s])
                        else:
                            arrived(there, self.buf.at[s], self.sem.at[s])

    spread_q = Spread("q", wq, sem_q)
    spread_kv = Spread("k", wkv, sem_kv)
    spread_p = Spread("p", wp, sem_p, 1.0)
    spread_a = Spread("a", wa, sem_a, 1.0)
    spread_b = Spread("b", wb, sem_b, 0.5, sem_b_side)
    for copy in locals_[:n_in]:
        copy.wait()
    for spread in (spread_q, spread_kv, spread_p):
        spread.begin_z()
        spread.begin_x()
    locals_[n_in].wait()

    mine = pl.ds(pl.multiple_of(t * rows, rows), rows)
    wide = tokv[...].astype(F32)
    inverse = lax.rsqrt(jnp.mean(wide * wide, axis=1, keepdims=True) + EPS)
    piece = xs.shape[2]
    for i in range(n_sp):
        span = slice(i * piece, (i + 1) * piece)
        xs[i, mine, :] = (tokv[:, span].astype(F32) * inverse * gain[:, span]).astype(BF16)

    def rows_of(device):
        return xs.at[:, pl.ds(pl.multiple_of(device * rows, rows), rows), :]

    for d in range(1, chips):
        send(None, rows_of(t), rows_of(t), sem_tok.at[t], (me, (y + d) % chips * CORES + c))
    send(None, rows_of(t), rows_of(t), sem_tok.at[t], (me, partner))

    def chip_rows(chip):
        return pl.ds(pl.multiple_of(chip * per, per), per)

    near = [y]
    far = [(y + d) % chips for d in range(1, chips)]

    def project(spread, at, h, which):
        spread.take(h)
        w = spread.buf.shape[2]
        with jax.named_scope(f"m{spread.name}{h}"):
            for level, there, _, _ in at_distance(h):

                def run(level=level):
                    for chip in which:
                        r = chip_rows(chip)
                        value = None
                        for i in range(cols):
                            s = level * cols + i
                            part = jnp.dot(
                                xs[s, r, :], spread.buf[s], preferred_element_type=F32
                            )
                            value = part if value is None else value + part
                        if h == 0:
                            acc[r, at : at + w] = value
                        else:
                            acc[r, at : at + w] += value

                when(there, run)

    def project_q(h, which):
        project(spread_q, 0, h, which)

    def project_kv(h, which):
        project(spread_kv, qw, h, which)

    def project_p(h, which):
        project(spread_p, channel0, h, which)

    arrived(None, rows_of(partner), sem_tok.at[partner])
    for copy in locals_[n_in + 1 :]:
        copy.wait()

    def gather_tokens():
        with jax.named_scope("tokf"):
            for d in range(1, chips):
                at = (y + chips - d) % chips * CORES + c
                arrived(None, rows_of(at), sem_tok.at[at])
                send(None, rows_of(at), rows_of(at), sem_tok.at[at], (me, partner))

    def take_tokens():
        with jax.named_scope("tokt"):
            for d in range(1, chips):
                at = (y + chips - d) % chips * CORES + (1 - c)
                arrived(None, rows_of(at), sem_tok.at[at])

    last = levels - 1
    for h in range(1, last):
        spread_q.forward(h)
        if h > 1:
            project_p(h - 2, near)
        spread_kv.forward(h)
        project_q(h - 1, near)
        spread_p.forward(h)
        project_kv(h - 1, near)
    spread_p.forward_side()
    spread_a.begin_z()
    gather_tokens()
    done = max(0, last - 1)
    if last:
        spread_q.forward(last)
    take_tokens()
    for h in range(done):
        project_q(h, far)
        project_kv(h, far)
    for h in range(max(0, last - 2)):
        project_p(h, far)
    if last:
        spread_kv.forward(last)
    for h in range(done, last):
        project_q(h, near + far)
        project_kv(h, near + far)
    if last:
        spread_p.forward(last)
    for h in range(max(0, last - 2), last):
        if h != 1:
            project_p(h, near + far)
    project_q(last, far + near)
    project_kv(last, far + near)

    def settle(lo, hi):
        for chip in range(chips):
            r = slice(chip * per, (chip + 1) * per)
            ext[WINDOW + chip * per : WINDOW + (chip + 1) * per, lo:hi] = acc[r, lo:hi].astype(BF16)

    with jax.named_scope("settleq"):
        settle(0, channel0)

    def pass_on(cond, at, width, n, i):
        head = ext.at[pl.ds(WINDOW - n, n), pl.ds(at, width)]
        tail = ext.at[pl.ds(seq + WINDOW - n, n), pl.ds(at, width)]
        send(both(cond, later), tail, head, sem_halo.at[i], (me + 1, t))
        return head

    head_kv = pass_on(None, qw, kw + vw, WINDOW, 0)
    spread_a.begin_x()
    spread_b.begin_z()

    group_heads = qw // kw
    stacked = group_heads * WINDOW
    scale = HEAD_DIM ** (-0.5)

    def attend(n):
        q_rows = pl.ds(pl.multiple_of(n * WINDOW + WINDOW, WINDOW), WINDOW)
        k_rows = pl.ds(pl.multiple_of(n * WINDOW, WINDOW), 2 * WINDOW)
        queries = ext[q_rows, :qw]
        keys = ext[k_rows, qw : qw + kw]
        values = ext[k_rows, qw + kw : channel0]
        row = lax.broadcasted_iota(jnp.int32, (stacked, 2 * WINDOW), 0)
        q_index = row % WINDOW
        k_index = lax.broadcasted_iota(jnp.int32, (stacked, 2 * WINDOW), 1)
        lowest = jnp.where(me * blocks + n == 0, WINDOW, 0)
        allowed = (k_index > q_index) & (k_index <= q_index + WINDOW) & (k_index >= lowest)
        which = lax.broadcasted_iota(jnp.int32, (stacked, 1), 0) // WINDOW
        done = []
        for j in range(kw // HEAD_DIM):
            part = slice(j * HEAD_DIM, (j + 1) * HEAD_DIM)
            first = j * group_heads
            q = jnp.concatenate(
                [
                    queries[:, (first + g) * HEAD_DIM : (first + g + 1) * HEAD_DIM]
                    for g in range(group_heads)
                ],
                axis=0,
            )
            scores = (
                lax.dot_general(
                    q, keys[:, part], (((1,), (1,)), ((), ())), preferred_element_type=F32
                )
                * scale
            )
            scores = jnp.where(allowed, scores, -jnp.inf)
            sinks = jnp.full((stacked, 1), sink[first], F32)
            for g in range(1, group_heads):
                sinks = jnp.where(which == g, sink[first + g], sinks)
            peak = jnp.maximum(jnp.max(scores, axis=1, keepdims=True), sinks)
            expo = jnp.exp(scores - peak)
            denom = jnp.sum(expo, axis=1, keepdims=True) + jnp.exp(sinks - peak)
            probs = (expo * (1.0 / denom)).astype(BF16)
            got = jnp.dot(probs, values[:, part], preferred_element_type=F32)
            done += [got[g * WINDOW : (g + 1) * WINDOW] for g in range(group_heads)]
        to = pl.ds(pl.multiple_of(n * WINDOW, WINDOW), WINDOW)
        mix[to, :qw] = jnp.concatenate(done, axis=1).astype(BF16)

    group = t * pw // POOL_CH
    whole_prefix = group == POOL_GROUPS - 1

    third = max(2, 2 * blocks // 3)
    with jax.named_scope("att1"):
        pl.loop(1, third)(attend)
    if last:
        spread_a.forward(1)
    if last >= 1:
        for h in sorted({1, last}):
            project_p(h, far + near)
    with jax.named_scope("settlep"):
        settle(channel0, ext.shape[1])
    heads_pool = []
    for g, reach in enumerate(SHORT_REACHES + (WINDOW,)):
        n = -(-(reach - 1) // 16) * 16
        heads_pool.append((group == g, pass_on(group == g, channel0, pw, n, 1)))
    total = jnp.sum(ext[WINDOW:, channel0:].astype(F32), axis=0, keepdims=True)
    tot[me] = jnp.broadcast_to(total, tot.shape[1:])
    for d in range(1, n_sp):
        send(
            both(whole_prefix, me + d < n_sp), tot.at[me], tot.at[me], sem_tot.at[me],
            (me + d, t),
        )
    spread_b.begin_x()
    if last:
        spread_b.forward(1)
    with jax.named_scope("att2"):
        pl.loop(third, blocks)(attend)
    with jax.named_scope("halokv"):
        arrived(earlier, head_kv, sem_halo.at[0])
    with jax.named_scope("att0"):
        attend(0)
    if last >= 2:
        spread_a.forward(2)
    with jax.named_scope("halopool"):
        for cond, head in heads_pool:
            arrived(both(cond, earlier), head, sem_halo.at[1])
    carry[...] = jnp.zeros(carry.shape, F32)
    for d in range(1, n_sp):

        def add(d=d):
            arrived(None, tot.at[me - d], sem_tot.at[me - d])
            carry[...] += tot[me - d]

        when(both(whole_prefix, me - d >= 0), add)

    reach = jnp.where(
        group == 0, SHORT_REACHES[0], jnp.where(group == 1, SHORT_REACHES[1], WINDOW)
    )
    reach = jnp.where(whole_prefix, n_sp * seq, reach)
    lowest = jnp.where(whole_prefix, WINDOW, 0)
    scope = jax.named_scope("pool")
    scope.__enter__()

    @pl.loop(0, blocks)
    def _(n):
        q_index = lax.broadcasted_iota(jnp.int32, (WINDOW, 2 * WINDOW), 0)
        k_index = lax.broadcasted_iota(jnp.int32, (WINDOW, 2 * WINDOW), 1)
        distance = q_index + WINDOW - k_index
        band = (distance >= 0) & (distance < reach) & (k_index >= lowest)
        band = jnp.where(band, 1.0, 0.0).astype(BF16)
        k_rows = pl.ds(pl.multiple_of(n * WINDOW, WINDOW), 2 * WINDOW)
        both_blocks = ext[k_rows, channel0:]
        sums = jnp.dot(band, both_blocks, preferred_element_type=F32) + carry[0:1, :]
        position = me * seq + n * WINDOW + lax.broadcasted_iota(jnp.int32, (WINDOW, 1), 0)
        counted = jnp.minimum(position + 1, reach).astype(F32)
        mixed = (sums / counted - both_blocks[WINDOW:].astype(F32)) * pgain[...]
        mix[pl.ds(pl.multiple_of(n * WINDOW, WINDOW), WINDOW), qw:] = mixed.astype(BF16)
        carry[...] = jnp.where(
            whole_prefix, jnp.broadcast_to(sums[WINDOW - 1 :], carry.shape), 0.0
        )

    scope.__exit__(None, None, None)

    def product(s, chip, core):
        r = pl.ds(pl.multiple_of((chip * CORES + core) * rows, rows), rows)
        return jnp.dot(mix[r, :qw], wa[s], preferred_element_type=F32) + jnp.dot(
            mix[r, qw:], wb[s], preferred_element_type=F32
        )

    def multiply(tag, cond, s):
        def give():
            for i, chip in enumerate(far):
                dfar[s, i] = product(s, chip, 1 - c).astype(BF16)

        def give_near():
            dnear[s] = product(s, y, 1 - c).astype(BF16)

        def keep():
            for i, chip in enumerate(far):
                ofar[s, i] = product(s, chip, c)

        def keep_near():
            onear[s] = product(s, y, c)

        with jax.named_scope(f"mul{tag}"):
            if chips > 1:
                when(cond, give)
                send(cond, dfar.at[s], rfar.at[s], sem_far.at[s], (me, partner))
                when(cond, keep)
            when(cond, give_near)
            send(cond, dnear.at[s], rnear.at[s], sem_near.at[s], (me, partner))
            when(cond, keep_near)
        if chips == 1:
            return
        with jax.named_scope(f"fin{tag}"):
            arrived(cond, rfar.at[s], sem_far.at[s])

            def pack():
                for i in range(chips - 1):
                    ysend[s, i] = (ofar[s, i] + rfar[s, i].astype(F32)).astype(BF16)

            when(cond, pack)
            for i, chip in enumerate(far):
                send(
                    cond, ysend.at[s, i], yrecv.at[s, i], sem_y.at[s, i], (me, chip * CORES + c)
                )

    order = []

    def column(h):
        for i, (level, there, _, _) in enumerate(at_distance(h)):
            order.append((there, level * cols + x))
            multiply(f"c{h}_{i}", there, level * cols + x)

    def others(h):
        spread_a.take(h)
        spread_b.take(h)
        for i, (level, there, _, _) in enumerate(at_distance(h)):
            for s in spread_a.peers(level):
                order.append((there, s))
                multiply(f"o{h}_{i}", there, s)

    column(0)
    if last >= 2:
        spread_b.forward(2)
    spread_a.forward_side()
    spread_b.forward_side()
    if last:
        column(1)
    if last >= 3:
        spread_a.forward(3)
    others(0)
    if last >= 3:
        spread_b.forward(3)
    for h in range(2, last):
        column(h)
        others(h)
    if last > 1:
        column(last)
    if last:
        others(1)
    if last > 1:
        others(last)

    with jax.named_scope("final"):
        w = wa.shape[2]
        for cond, s in order:

            def end(s=s):
                arrived(None, rnear.at[s], sem_near.at[s])
                value = onear[s] + rnear[s].astype(F32)
                for i in range(chips - 1):
                    arrived(None, yrecv.at[s, i], sem_y.at[s, i])
                    value += yrecv[s, i].astype(F32)
                out[:, pl.ds(pl.multiple_of(s * w, w), w)] = value.astype(BF16)

            when(cond, end)

    with jax.named_scope("wsend"):
        for item in slots:
            if item is not None:
                when(item[0], item[1].wait_send)


def local(
    n_sp, n_tp, tokens_in, norm_gain, query_weight, key_weight, value_weight, pool_weight,
    sink_logit, pool_gain, attention_out_weight, pool_out_weight,
):
    rows, depth = tokens_in.shape
    seq = rows * n_tp
    ins = [query_weight, key_weight, value_weight, pool_weight]
    outs = [attention_out_weight, pool_out_weight]
    widths = tuple(w.shape[1] for w in ins)
    if widths[1] % 128:
        ins = [ins[0], jnp.concatenate(ins[1:3], axis=1), ins[3]]
    cols = math.gcd(n_sp, max(1, n_tp // CORES))
    chips = n_tp // CORES
    k_in, out_cols = ins[0].shape[0], outs[0].shape[1]
    width, others = sum(widths), max(1, chips - 1)
    qw, kw, vw, pw = widths
    vmem = pl.BlockSpec(memory_space=pltpu.VMEM)
    hbm = pl.BlockSpec(memory_space=pl.ANY)
    dma = pltpu.SemaphoreType.DMA
    return pl.pallas_call(
        functools.partial(kernel, n_sp, n_tp, cols, len(ins), len(outs), widths),
        out_shape=pltpu.VMEM((rows, depth), BF16),
        in_specs=[hbm, vmem, pl.BlockSpec(memory_space=pltpu.SMEM), vmem]
        + [hbm] * (len(ins) + len(outs)),
        out_specs=vmem,
        scratch_shapes=[
            pltpu.VMEM((rows, depth), BF16),
            pltpu.VMEM((n_sp, seq, depth // n_sp), BF16),
            pltpu.VMEM((n_sp, k_in, qw), BF16),
            pltpu.VMEM((n_sp, k_in, kw + vw), BF16),
            pltpu.VMEM((n_sp, k_in, pw), BF16),
            pltpu.VMEM((n_sp, outs[0].shape[0], out_cols), BF16),
            pltpu.VMEM((n_sp, outs[1].shape[0], out_cols), BF16),
            pltpu.VMEM((seq, width), F32),
            pltpu.VMEM((seq + WINDOW, width), BF16),
            pltpu.VMEM((seq, qw + pw), BF16),
            pltpu.VMEM((n_sp, 8, pw), F32),
            pltpu.VMEM((8, pw), F32),
            pltpu.VMEM((n_sp, others, rows, out_cols), BF16),
            pltpu.VMEM((n_sp, others, rows, out_cols), BF16),
            pltpu.VMEM((n_sp, rows, out_cols), BF16),
            pltpu.VMEM((n_sp, rows, out_cols), BF16),
            pltpu.VMEM((n_sp, others, rows, out_cols), BF16),
            pltpu.VMEM((n_sp, others, rows, out_cols), BF16),
            pltpu.VMEM((n_sp, others, rows, out_cols), F32),
            pltpu.VMEM((n_sp, rows, out_cols), F32),
            dma((len(ins) + len(outs) + 1,)),
            dma((SEND_SLOTS,)),
            dma((n_sp,)),
            dma((n_sp,)),
            dma((n_sp,)),
            dma((n_sp,)),
            dma((n_sp,)),
            dma((n_sp,)),
            dma((n_tp,)),
            dma((2,)),
            dma((n_sp,)),
            dma((n_sp,)),
            dma((n_sp,)),
            dma((n_sp, others)),
        ],
        compiler_params=pltpu.CompilerParams(
            collective_id=0, has_side_effects=True, vmem_limit_bytes=58 << 20
        ),
    )(
        tokens_in, norm_gain.reshape(1, -1), sink_logit, pool_gain.reshape(1, -1), *ins, *outs
    )


def solution(mesh):
    in_specs = (
        P(("sp", "tp"), None), P(), P("sp", "tp"), P("sp", "tp"), P("sp", "tp"), P("sp", "tp"),
        P("tp"), P("tp"), P("tp", "sp"), P("tp", "sp"),
    )
    out_specs = P(("sp", "tp"), None)
    return jax.shard_map(
        functools.partial(local, mesh.shape["sp"], mesh.shape["tp"]),
        mesh=mesh, in_specs=in_specs, out_specs=out_specs, check_vma=False,
    )
```

```python
import functools
import math

import jax
import jax.numpy as jnp
from jax import lax
from jax.experimental import pallas as pl
from jax.experimental.pallas import tpu as pltpu
from jax.sharding import PartitionSpec as P

HEAD_DIM = 64
POOL_CH = 256
POOL_GROUPS = 4
WINDOW = 128
EPS = 1e-06
SHORT_REACHES = (8, 32)
CORES = 2
SEND_SLOTS = 40
MESH = pl.DeviceIdType.MESH
F32 = jnp.float32
BF16 = jnp.bfloat16


def when(cond, fn):
    if cond is None:
        fn()
    else:
        pl.when(cond)(fn)


def both(a, b):
    return b if a is None else (a if b is None else jnp.logical_and(a, b))


def kernel(n_sp, n_tp, cols, n_in, n_out, widths, *refs):
    tok, gain_in, sink_in, pgain_in = refs[:4]
    win_refs = refs[4 : 4 + n_in]
    wout_refs = refs[4 + n_in : 4 + n_in + n_out]
    (
        out, tokv, xs, wq, wkv, wp, wa, wb, acc, ext, mix, tot, carry, given, dfar, rfar, dnear, rnear,
        ysend, yrecv, ofar, onear, gain, pgain, sink,
        local_sem, send_sem, once_sem, sem_q, sem_kv, sem_p, sem_a, sem_b, sem_a_side,
        sem_tok, sem_halo, sem_tot, sem_far, sem_near, sem_y,
    ) = refs[4 + n_in + n_out :]
    qw, kw, vw, pw = widths
    levels = n_sp // cols
    chips = n_tp // CORES
    rows, seq = tok.shape[0], xs.shape[1]
    per = rows * CORES
    channel0 = qw + kw + vw
    blocks = seq // WINDOW
    me, t = lax.axis_index("sp"), lax.axis_index("tp")
    z, x = me // cols, me % cols
    y, c = t // CORES, t % CORES
    partner = y * CORES + (1 - c)
    up, down = z + 1 < levels, z > 0
    later, earlier = me + 1 < n_sp, me > 0
    last = levels - 1
    at_end = jnp.logical_or(z == 0, z == last)
    inner = jnp.logical_not(at_end)

    ext[:WINDOW, qw:] = jnp.zeros((WINDOW, ext.shape[1] - qw), BF16)

    barrier = pltpu.get_barrier_semaphore()
    next_row = jnp.logical_and(x == cols - 1, up)
    last_row = jnp.logical_and(x == 0, down)

    def greet(cond, sp, tp):
        when(
            cond,
            lambda: pl.semaphore_signal(
                barrier, inc=1, device_id=(sp, tp), device_id_type=MESH
            ),
        )

    for d in range(1, cols):
        greet(None, z * cols + (x + d) % cols, t)
    greet(up, me + cols, t)
    greet(down, me - cols, t)
    greet_diagonal = cols > 1
    if greet_diagonal:
        greet(next_row, me + 1, t)
        greet(last_row, me - 1, t)
    for d in range(1, n_tp):
        greet(None, me, (t + d) % n_tp)
    expected = cols - 1 + n_tp - 1 + jnp.where(up, 1, 0) + jnp.where(down, 1, 0)
    if greet_diagonal:
        expected = expected + jnp.where(next_row, 1, 0) + jnp.where(last_row, 1, 0)
    locals_ = []

    def fetch(src, dst):
        copy = pltpu.make_async_copy(src, dst, local_sem.at[len(locals_)])
        copy.start()
        locals_.append(copy)

    fetch(win_refs[0], wq.at[me])
    at = 0
    for ref in win_refs[1:-1]:
        w = ref.shape[1]
        fetch(ref, wkv.at[me, :, pl.ds(at, w)])
        at += w
    fetch(win_refs[-1], wp.at[me])
    fetch(tok, tokv)
    fetch(gain_in, gain)
    fetch(wout_refs[0], wa.at[me])
    fetch(wout_refs[1], wb.at[me])
    fetch(pgain_in, pgain)
    fetch(sink_in, sink)
    with jax.named_scope("barrier"):
        pl.semaphore_wait(barrier, expected)

    slots = [None] * send_sem.shape[0]
    count = [0]

    def send(cond, src, dst, recv, dev):
        slot = count[0] % len(slots)
        count[0] += 1
        if slots[slot] is not None:
            when(slots[slot][0], slots[slot][1].wait_send)
        copy = pltpu.make_async_remote_copy(
            src_ref=src, dst_ref=dst, send_sem=send_sem.at[slot], recv_sem=recv,
            device_id=dev, device_id_type=MESH,
        )
        when(cond, copy.start)
        slots[slot] = (cond, copy)

    fixed = []

    def send_once(cond, src, dst, sem, recv, dev):
        copy = pltpu.make_async_remote_copy(
            src_ref=src, dst_ref=dst, send_sem=sem, recv_sem=recv, device_id=dev,
            device_id_type=MESH,
        )
        when(cond, copy.start)
        fixed.append((cond, copy))

    def arrived(cond, dst, recv):
        copy = pltpu.make_async_remote_copy(
            src_ref=dst, dst_ref=dst, send_sem=send_sem.at[0], recv_sem=recv,
            device_id=(me, partner), device_id_type=MESH,
        )
        when(cond, copy.wait_recv)

    def at_distance(h):
        if h == 0:
            return ((z, None, None, None),)
        return (
            (z - h, z - h >= 0, up, me + cols),
            (z + h, z + h < levels, down, me - cols),
        )

    class Spread:
        def __init__(
            self, name, buf, sem, share=0.0, side_sem=None, ends=False, next_too=False
        ):
            self.name, self.buf, self.sem, self.side_sem = name, buf, sem, side_sem
            k = buf.shape[1]
            self.side = int(k * share) // 16 * 16 if cols > 1 and levels > 1 else 0
            self.k, self.ends, self.next_too = k, ends, next_too and cols > 1 and last > 1
            self.have, self.have_at_ends = set(), set()

        def piece(self, s, lo, hi):
            return self.buf.at[s] if (lo, hi) == (0, self.k) else self.buf.at[s, pl.ds(lo, hi - lo), :]

        def side_at(self, h):
            return self.side if h == (last if self.ends else 1) else 0

        def side_sems(self):
            return self.sem if self.side == self.k else self.side_sem

        def go(self, cond, s, lo, hi, sem, dev_sp):
            ref = self.piece(s, lo, hi)
            send(cond, ref, ref, sem.at[s], (dev_sp, t))

        def across(self, cond, s, lo=0):
            if lo == self.k:
                return
            for d in range(1, cols):
                self.go(cond, s, lo, self.k, self.sem, z * cols + (x + d) % cols)

        def begin_up(self, cond=None):
            self.go(both(up, cond), me, 0, self.k, self.sem, me + cols)

        def begin_down(self):
            self.go(down, me, 0, self.k, self.sem, me - cols)

        def begin_x(self, cond=None):
            self.across(cond, me)

        def forward(self, h, cond=None):
            with jax.named_scope(f"f{self.name}{h}"):
                for level, there, on, to in at_distance(h):
                    there = both(there, cond)
                    s = level * cols + x
                    arrived(there, self.buf.at[s], self.sem.at[s])
                    self.go(both(there, on), s, 0, self.k, self.sem, to)
                    if self.next_too and h == 1:
                        there = both(there, jnp.logical_and(level != 0, level != last))
                    self.across(there, s, self.side_at(h))

        def peers(self, level):
            return [level * cols + (x + cols - d) % cols for d in range(1, cols)]

        def forward_side(self):
            if not self.side:
                return
            if not self.ends:
                self.take(0)
            sem = self.side_sems()
            for s in self.peers(z):
                if not self.ends:
                    self.go(up, s, 0, self.side, sem, me + cols)
                    self.go(down, s, 0, self.side, sem, me - cols)
                    continue
                self.go(at_end, s, 0, self.side, sem, (last - z) * cols + x)

        def forward_next(self):
            if not self.next_too:
                return
            self.take(0, at_end)
            for s in self.peers(z):
                self.go(z == 0, s, 0, self.k, self.sem, me + cols)
                self.go(z == last, s, 0, self.k, self.sem, me - cols)

        def take(self, h, cond=None):
            if h in self.have or (h in self.have_at_ends and cond is at_end):
                return
            if cond is at_end:
                self.have_at_ends.add(h)
            else:
                self.have.add(h)
                cond = inner if h in self.have_at_ends else cond
            side = self.side_at(h)
            with jax.named_scope(f"t{self.name}{h}"):
                for level, there, _, _ in at_distance(h):
                    there = both(there, cond)
                    for s in self.peers(level):
                        if side:
                            arrived(there, self.piece(s, 0, side), self.side_sems().at[s])
                        if side < self.k:
                            arrived(there, self.piece(s, side, self.k), self.sem.at[s])

    spread_q = Spread("q", wq, sem_q, next_too=True)
    spread_kv = Spread("k", wkv, sem_kv, next_too=True)
    spread_p = Spread("p", wp, sem_p, 1.0)
    spread_a = Spread("a", wa, sem_a, 0.5, sem_a_side, True, True)
    spread_b = Spread("b", wb, sem_b, 1.0, None, True, True)
    for copy in locals_[:n_in]:
        copy.wait()
    for spread in (spread_q, spread_kv, spread_p):
        spread.begin_up()
        spread.begin_down()
        spread.begin_x()
    locals_[n_in].wait()
    locals_[n_in + 1].wait()

    mine = pl.ds(pl.multiple_of(t * rows, rows), rows)
    wide = tokv[...].astype(F32)
    inverse = lax.rsqrt(jnp.mean(wide * wide, axis=1, keepdims=True) + EPS)
    piece = xs.shape[2]
    for i in range(n_sp):
        span = slice(i * piece, (i + 1) * piece)
        xs[i, mine, :] = (tokv[:, span].astype(F32) * inverse * gain[:, span]).astype(BF16)

    def rows_of(device):
        return xs.at[:, pl.ds(pl.multiple_of(device * rows, rows), rows), :]

    for d in range(1, chips):
        send(None, rows_of(t), rows_of(t), sem_tok.at[t], (me, (y + d) % chips * CORES + c))
    send(None, rows_of(t), rows_of(t), sem_tok.at[t], (me, partner))

    def chip_rows(chip):
        return pl.ds(pl.multiple_of(chip * per, per), per)

    near = [y]
    far = [(y + d) % chips for d in range(1, chips)]

    def project(spread, at, h, which):
        spread.take(h)
        w = spread.buf.shape[2]
        with jax.named_scope(f"m{spread.name}{h}"):
            for level, there, _, _ in at_distance(h):

                def run(level=level):
                    for chip in which:
                        r = chip_rows(chip)
                        value = None
                        for i in range(cols):
                            s = level * cols + i
                            part = jnp.dot(
                                xs[s, r, :], spread.buf[s], preferred_element_type=F32
                            )
                            value = part if value is None else value + part
                        if h == 0:
                            acc[r, at : at + w] = value
                        else:
                            acc[r, at : at + w] += value

                when(there, run)

    def project_q(h, which):
        project(spread_q, 0, h, which)

    def project_kv(h, which):
        project(spread_kv, qw, h, which)

    def project_p(h, which):
        project(spread_p, channel0, h, which)

    arrived(None, rows_of(partner), sem_tok.at[partner])
    for copy in locals_[n_in + 2 :]:
        copy.wait()

    def gather_tokens():
        with jax.named_scope("tokf"):
            for d in range(1, chips):
                at = (y + chips - d) % chips * CORES + c
                arrived(None, rows_of(at), sem_tok.at[at])
                send(None, rows_of(at), rows_of(at), sem_tok.at[at], (me, partner))

    def take_tokens():
        with jax.named_scope("tokt"):
            for d in range(1, chips):
                at = (y + chips - d) % chips * CORES + (1 - c)
                arrived(None, rows_of(at), sem_tok.at[at])

    for h in range(1, last):
        spread_q.forward(h)
        if h > 1:
            project_p(h - 2, near)
        spread_kv.forward(h)
        if h == 1:
            spread_q.forward_next()
        project_q(h - 1, near)
        spread_p.forward(h)
        if h == 1:
            spread_kv.forward_next()
        project_kv(h - 1, near)
    spread_p.forward_side()
    spread_a.begin_down()
    spread_a.begin_up()
    spread_b.begin_down()
    spread_b.begin_up(at_end)
    gather_tokens()
    done = max(0, last - 1)
    if last:
        spread_q.forward(last)
    take_tokens()
    for h in range(done):
        project_q(h, far)
        project_kv(h, far)
    for h in range(max(0, last - 2)):
        project_p(h, far)
    if last:
        spread_kv.forward(last)
    for h in range(done, last):
        project_q(h, near + far)
        project_kv(h, near + far)
    if last:
        spread_p.forward(last)
    for h in range(max(0, last - 2), last):
        if h != 1:
            project_p(h, near + far)
    project_q(last, far + near)
    if last:
        project_p(1, far + near)
    project_kv(last, far + near)

    def settle(lo, hi):
        for chip in range(chips):
            r = slice(chip * per, (chip + 1) * per)
            ext[WINDOW + chip * per : WINDOW + (chip + 1) * per, lo:hi] = acc[r, lo:hi].astype(BF16)

    with jax.named_scope("settleq"):
        settle(0, channel0)

    def pass_on(cond, at, width, n, i):
        head = ext.at[pl.ds(WINDOW - n, n), pl.ds(at, width)]
        tail = ext.at[pl.ds(seq + WINDOW - n, n), pl.ds(at, width)]
        send_once(
            both(cond, later), tail, head, once_sem.at[i], sem_halo.at[i], (me + 1, t)
        )
        return head

    head_kv = pass_on(None, qw, kw + vw, WINDOW, 0)

    group = t * pw // POOL_CH
    whole_prefix = group == POOL_GROUPS - 1
    halos = [
        (group == g, -(-(reach - 1) // 16) * 16)
        for g, reach in enumerate(SHORT_REACHES + (WINDOW,))
    ]

    def finish_pool_rows(cond):
        def run():
            with jax.named_scope("settlep"):
                settle(channel0, ext.shape[1])
                for n in range(blocks):
                    r = slice(WINDOW + n * WINDOW, 2 * WINDOW + n * WINDOW)
                    total = jnp.sum(ext[r, channel0:].astype(F32), axis=0, keepdims=True)
                    if n + 1 < blocks:
                        carry[n + 1] = jnp.broadcast_to(
                            total if n == 0 else carry[n, 0:1, :] + total, carry.shape[1:]
                        )
                    else:
                        tot[me] = jnp.broadcast_to(
                            total if n == 0 else carry[n, 0:1, :] + total, tot.shape[1:]
                        )
                carry[0] = jnp.zeros(carry.shape[1:], F32)

        when(cond, run)
        for is_group, n in halos:
            pass_on(both(is_group, cond), channel0, pw, n, 1)
        for d in range(1, n_sp):
            send_once(
                both(both(whole_prefix, cond), me + d < n_sp), tot.at[me], tot.at[me],
                once_sem.at[1 + d], sem_tot.at[me], (me + d, t),
            )

    finish_pool_rows(inner)
    spread_a.begin_x()
    spread_b.begin_x(inner)
    spread_b.begin_up(inner)
    if last:
        spread_a.forward(1, inner)

    group_heads = qw // kw
    stacked = group_heads * WINDOW
    scale = HEAD_DIM ** (-0.5)

    def attend(n):
        q_rows = pl.ds(pl.multiple_of(n * WINDOW + WINDOW, WINDOW), WINDOW)
        k_rows = pl.ds(pl.multiple_of(n * WINDOW, WINDOW), 2 * WINDOW)
        queries = ext[q_rows, :qw]
        keys = ext[k_rows, qw : qw + kw]
        values = ext[k_rows, qw + kw : channel0]
        row = lax.broadcasted_iota(jnp.int32, (stacked, 2 * WINDOW), 0)
        q_index = row % WINDOW
        k_index = lax.broadcasted_iota(jnp.int32, (stacked, 2 * WINDOW), 1)
        lowest = jnp.where(me * blocks + n == 0, WINDOW, 0)
        allowed = (k_index > q_index) & (k_index <= q_index + WINDOW) & (k_index >= lowest)
        which = lax.broadcasted_iota(jnp.int32, (stacked, 1), 0) // WINDOW
        done = []
        for j in range(kw // HEAD_DIM):
            part = slice(j * HEAD_DIM, (j + 1) * HEAD_DIM)
            first = j * group_heads
            q = jnp.concatenate(
                [
                    queries[:, (first + g) * HEAD_DIM : (first + g + 1) * HEAD_DIM]
                    for g in range(group_heads)
                ],
                axis=0,
            )
            scores = (
                lax.dot_general(
                    q, keys[:, part], (((1,), (1,)), ((), ())), preferred_element_type=F32
                )
                * scale
            )
            scores = jnp.where(allowed, scores, -jnp.inf)
            sinks = jnp.full((stacked, 1), sink[first], F32)
            for g in range(1, group_heads):
                sinks = jnp.where(which == g, sink[first + g], sinks)
            peak = jnp.maximum(jnp.max(scores, axis=1, keepdims=True), sinks)
            expo = jnp.exp(scores - peak)
            denom = jnp.sum(expo, axis=1, keepdims=True) + jnp.exp(sinks - peak)
            probs = (expo * (1.0 / denom)).astype(BF16)
            got = jnp.dot(probs, values[:, part], preferred_element_type=F32)
            done += [got[g * WINDOW : (g + 1) * WINDOW] for g in range(group_heads)]
        to = pl.ds(pl.multiple_of(n * WINDOW, WINDOW), WINDOW)
        mix[to, :qw] = jnp.concatenate(done, axis=1).astype(BF16)

    if per % WINDOW == 0:
        span = per // WINDOW
        far_blocks, near_blocks = [chip * span for chip in far], [y * span]
    else:
        span = blocks
        far_blocks, near_blocks = [0], []

    def attend_later_blocks(firsts):
        with jax.named_scope("att"):
            for first in firsts:
                pl.loop(1, span)(lambda i, first=first: attend(first + i))

    def attend_first_block(firsts):
        with jax.named_scope("att0"):
            for first in firsts:
                cond = earlier if isinstance(first, int) else both(earlier, first == 0)
                arrived(cond, head_kv, sem_halo.at[0])
                attend(first)

    reach = jnp.where(
        group == 0, SHORT_REACHES[0], jnp.where(group == 1, SHORT_REACHES[1], WINDOW)
    )
    reach = jnp.where(whole_prefix, n_sp * seq, reach)
    lowest = jnp.where(whole_prefix, WINDOW, 0)

    def pool(firsts):
        with jax.named_scope("pool"):
            for first in firsts:

                @pl.loop(0, span)
                def _(i, first=first):
                    n = first + i
                    q_index = lax.broadcasted_iota(jnp.int32, (WINDOW, 2 * WINDOW), 0)
                    k_index = lax.broadcasted_iota(jnp.int32, (WINDOW, 2 * WINDOW), 1)
                    distance = q_index + WINDOW - k_index
                    band = (distance >= 0) & (distance < reach) & (k_index >= lowest)
                    band = jnp.where(band, 1.0, 0.0).astype(BF16)
                    k_rows = pl.ds(pl.multiple_of(n * WINDOW, WINDOW), 2 * WINDOW)
                    both_blocks = ext[k_rows, channel0:]
                    before = jnp.where(whole_prefix, carry[n, 0:1, :] + given[0:1, :], 0.0)
                    sums = jnp.dot(band, both_blocks, preferred_element_type=F32) + before
                    position = (
                        me * seq + n * WINDOW + lax.broadcasted_iota(jnp.int32, (WINDOW, 1), 0)
                    )
                    counted = jnp.minimum(position + 1, reach).astype(F32)
                    mixed = (sums / counted - both_blocks[WINDOW:].astype(F32)) * pgain[...]
                    to = pl.ds(pl.multiple_of(n * WINDOW, WINDOW), WINDOW)
                    mix[to, qw:] = mixed.astype(BF16)

    attend_later_blocks(far_blocks)
    if last >= 2:
        project_p(last, far + near)
    finish_pool_rows(at_end)
    spread_b.begin_x(at_end)
    if last:
        spread_a.forward(1, at_end)
        spread_b.forward(1, inner)
    attend_first_block(far_blocks)
    if last:
        spread_b.forward(1, at_end)
    spread_a.forward_next()
    with jax.named_scope("halopool"):
        for cond, n in halos:
            head = ext.at[pl.ds(WINDOW - n, n), pl.ds(channel0, pw)]
            arrived(both(cond, earlier), head, sem_halo.at[1])
        given[...] = jnp.zeros(given.shape, F32)
        for d in range(1, n_sp):

            def add(d=d):
                arrived(None, tot.at[me - d], sem_tot.at[me - d])
                given[...] += tot[me - d]

            when(both(whole_prefix, me - d >= 0), add)
    pool(far_blocks)

    def product(s, chip, core):
        r = pl.ds(pl.multiple_of((chip * CORES + core) * rows, rows), rows)
        return jnp.dot(mix[r, :qw], wa[s], preferred_element_type=F32) + jnp.dot(
            mix[r, qw:], wb[s], preferred_element_type=F32
        )

    def column(h):
        return [(there, level * cols + x) for level, there, _, _ in at_distance(h)]

    def others(h):
        return [
            (there, s)
            for level, there, _, _ in at_distance(h)
            for s in spread_a.peers(level)
        ]

    def multiply_far(pieces):
        for cond, s in pieces if chips > 1 else ():

            def give(s=s):
                for i, chip in enumerate(far):
                    dfar[s, i] = product(s, chip, 1 - c).astype(BF16)

            def keep(s=s):
                for i, chip in enumerate(far):
                    ofar[s, i] = product(s, chip, c)

            with jax.named_scope("mulf"):
                when(cond, give)
                send(cond, dfar.at[s], rfar.at[s], sem_far.at[s], (me, partner))
                when(cond, keep)

    def multiply_near(pieces):
        for cond, s in pieces:

            def give_near(s=s):
                dnear[s] = product(s, y, 1 - c).astype(BF16)

            def keep_near(s=s):
                onear[s] = product(s, y, c)

            with jax.named_scope("muln"):
                when(cond, give_near)
                send(cond, dnear.at[s], rnear.at[s], sem_near.at[s], (me, partner))
                when(cond, keep_near)

    def finish(pieces):
        for cond, s in pieces if chips > 1 else ():

            def pack(s=s):
                for i in range(chips - 1):
                    ysend[s, i] = (ofar[s, i] + rfar[s, i].astype(F32)).astype(BF16)

            with jax.named_scope("fin"):
                arrived(cond, rfar.at[s], sem_far.at[s])
                when(cond, pack)
                for i, chip in enumerate(far):
                    send(
                        cond, ysend.at[s, i], yrecv.at[s, i], sem_y.at[s, i],
                        (me, chip * CORES + c),
                    )

    def multiply(pieces):
        for piece in pieces:
            multiply_far([piece])
            multiply_near([piece])
            finish([piece])

    first = column(0)
    second = column(1) if last else []
    third = others(0)
    multiply_far(first)
    multiply_far(second)
    finish(first)
    if last >= 2:
        spread_a.forward(2)
        spread_b.forward(2, inner)
    finish(second)
    attend_later_blocks(near_blocks)
    spread_b.forward_next()
    attend_first_block(near_blocks)
    if last >= 2:
        spread_b.forward(2, at_end)
    spread_a.take(0)
    spread_b.take(0)
    multiply_far(third)
    pool(near_blocks)
    finish(third)
    spread_b.forward_side()
    spread_a.forward_side()
    fourth = column(2) if last >= 2 else []
    multiply_far(fourth)
    multiply_near(first)
    finish(fourth)

    def only(cond, pieces):
        return [(both(there, cond), s) for there, s in pieces]

    order = first + second + third + fourth

    def take_others(h, cond):
        spread_a.take(h, cond)
        spread_b.take(h, cond)
        multiply(only(cond, others(h)))
        order.extend(only(cond, others(h)))

    if last > 1:
        take_others(1, at_end)
    if last >= 3:
        spread_a.forward(3)
    multiply_near(second)
    multiply_near(third)
    multiply_near(fourth)
    if last >= 3:
        spread_b.forward(3)
    for h in range(3, last + 1):
        multiply(column(h))
        order += column(h)
    for h in range(2, last):
        take_others(h, None)
    if last > 1:
        take_others(1, inner)
    if last:
        take_others(last, None)

    with jax.named_scope("final"):
        w = wa.shape[2]
        for cond, s in order:

            def end(s=s):
                arrived(None, rnear.at[s], sem_near.at[s])
                value = onear[s] + rnear[s].astype(F32)
                for i in range(chips - 1):
                    arrived(None, yrecv.at[s, i], sem_y.at[s, i])
                    value += yrecv[s, i].astype(F32)
                out[:, pl.ds(pl.multiple_of(s * w, w), w)] = value.astype(BF16)

            when(cond, end)

    with jax.named_scope("wsend"):
        for item in slots + fixed:
            if item is not None:
                when(item[0], item[1].wait_send)


def local(
    n_sp, n_tp, tokens_in, norm_gain, query_weight, key_weight, value_weight, pool_weight,
    sink_logit, pool_gain, attention_out_weight, pool_out_weight,
):
    rows, depth = tokens_in.shape
    seq = rows * n_tp
    ins = [query_weight, key_weight, value_weight, pool_weight]
    outs = [attention_out_weight, pool_out_weight]
    widths = tuple(w.shape[1] for w in ins)
    if widths[1] % 128:
        ins = [ins[0], jnp.concatenate(ins[1:3], axis=1), ins[3]]
    cols = math.gcd(n_sp, max(1, n_tp // CORES))
    chips = n_tp // CORES
    k_in, out_cols = ins[0].shape[0], outs[0].shape[1]
    width, others = sum(widths), max(1, chips - 1)
    qw, kw, vw, pw = widths
    vmem = pl.BlockSpec(memory_space=pltpu.VMEM)
    hbm = pl.BlockSpec(memory_space=pl.ANY)
    dma = pltpu.SemaphoreType.DMA
    return pl.pallas_call(
        functools.partial(kernel, n_sp, n_tp, cols, len(ins), len(outs), widths),
        out_shape=pltpu.VMEM((rows, depth), BF16),
        in_specs=[hbm] * (4 + len(ins) + len(outs)),
        out_specs=vmem,
        scratch_shapes=[
            pltpu.VMEM((rows, depth), BF16),
            pltpu.VMEM((n_sp, seq, depth // n_sp), BF16),
            pltpu.VMEM((n_sp, k_in, qw), BF16),
            pltpu.VMEM((n_sp, k_in, kw + vw), BF16),
            pltpu.VMEM((n_sp, k_in, pw), BF16),
            pltpu.VMEM((n_sp, outs[0].shape[0], out_cols), BF16),
            pltpu.VMEM((n_sp, outs[1].shape[0], out_cols), BF16),
            pltpu.VMEM((seq, width), F32),
            pltpu.VMEM((seq + WINDOW, width), BF16),
            pltpu.VMEM((seq, qw + pw), BF16),
            pltpu.VMEM((n_sp, 8, pw), F32),
            pltpu.VMEM((seq // WINDOW, 8, pw), F32),
            pltpu.VMEM((8, pw), F32),
            pltpu.VMEM((n_sp, others, rows, out_cols), BF16),
            pltpu.VMEM((n_sp, others, rows, out_cols), BF16),
            pltpu.VMEM((n_sp, rows, out_cols), BF16),
            pltpu.VMEM((n_sp, rows, out_cols), BF16),
            pltpu.VMEM((n_sp, others, rows, out_cols), BF16),
            pltpu.VMEM((n_sp, others, rows, out_cols), BF16),
            pltpu.VMEM((n_sp, others, rows, out_cols), F32),
            pltpu.VMEM((n_sp, rows, out_cols), F32),
            pltpu.VMEM((1, depth), F32),
            pltpu.VMEM((1, pw), F32),
            pltpu.SMEM(sink_logit.shape, F32),
            dma((len(ins) + len(outs) + 4,)),
            dma((SEND_SLOTS,)),
            dma((n_sp + 1,)),
            dma((n_sp,)),
            dma((n_sp,)),
            dma((n_sp,)),
            dma((n_sp,)),
            dma((n_sp,)),
            dma((n_sp,)),
            dma((n_tp,)),
            dma((2,)),
            dma((n_sp,)),
            dma((n_sp,)),
            dma((n_sp,)),
            dma((n_sp, others)),
        ],
        compiler_params=pltpu.CompilerParams(
            collective_id=0, has_side_effects=True, vmem_limit_bytes=58 << 20
        ),
    )(
        tokens_in, norm_gain.reshape(1, -1), sink_logit, pool_gain.reshape(1, -1), *ins, *outs
    )


def solution(mesh):
    in_specs = (
        P(("sp", "tp"), None), P(), P("sp", "tp"), P("sp", "tp"), P("sp", "tp"), P("sp", "tp"),
        P("tp"), P("tp"), P("tp", "sp"), P("tp", "sp"),
    )
    out_specs = P(("sp", "tp"), None)
    return jax.shard_map(
        functools.partial(local, mesh.shape["sp"], mesh.shape["tp"]),
        mesh=mesh, in_specs=in_specs, out_specs=out_specs, check_vma=False,
    )
```

```python
import functools
import math

import jax
import jax.numpy as jnp
from jax import lax
from jax.experimental import pallas as pl
from jax.experimental.pallas import tpu as pltpu
from jax.sharding import PartitionSpec as P

HEAD_DIM = 64
POOL_CH = 256
POOL_GROUPS = 4
WINDOW = 128
EPS = 1e-06
SHORT_REACHES = (8, 32)
CORES = 2
SEND_GROUPS = 19
SIDE_SHARE = 0.375
MESH = pl.DeviceIdType.MESH
F32 = jnp.float32
BF16 = jnp.bfloat16


def when(cond, fn):
    if cond is None:
        fn()
    else:
        pl.when(cond)(fn)


def both(a, b):
    return b if a is None else (a if b is None else jnp.logical_and(a, b))


def kernel(n_sp, n_tp, cols, n_in, n_out, widths, *refs):
    tok, gain_in, sink_in, pgain_in = refs[:4]
    win_refs = refs[4 : 4 + n_in]
    wout_refs = refs[4 + n_in : 4 + n_in + n_out]
    (
        out, tokv, xs, wq, wkv, wp, wa, wb, acc, ext, mix, tot, carry, given, dfar, rfar, dnear, rnear,
        ysend, yrecv, ofar, onear, gain, pgain, sink,
        local_sem, send_sem, sem_q, sem_kv, sem_p, sem_a, sem_b, sem_a_side,
        sem_tok, sem_halo, sem_tot, sem_far, sem_near, sem_y,
    ) = refs[4 + n_in + n_out :]
    qw, kw, vw, pw = widths
    levels = n_sp // cols
    chips = n_tp // CORES
    rows, seq = tok.shape[0], xs.shape[1]
    per = rows * CORES
    channel0 = qw + kw + vw
    blocks = seq // WINDOW
    me, t = lax.axis_index("sp"), lax.axis_index("tp")
    z, x = me // cols, me % cols
    y, c = t // CORES, t % CORES
    partner = y * CORES + (1 - c)
    up, down = z + 1 < levels, z > 0
    later, earlier = me + 1 < n_sp, me > 0
    last = levels - 1
    at_end = jnp.logical_or(z == 0, z == last)
    inner = jnp.logical_not(at_end)

    ext[:WINDOW, qw:] = jnp.zeros((WINDOW, ext.shape[1] - qw), BF16)

    barrier = pltpu.get_barrier_semaphore()
    def greet(cond, sp, tp):
        when(
            cond,
            lambda: pl.semaphore_signal(
                barrier, inc=1, device_id=(sp, tp), device_id_type=MESH
            ),
        )

    for d in range(1, cols):
        greet(None, z * cols + (x + d) % cols, t)
    greet(up, me + cols, t)
    greet(down, me - cols, t)
    greet(None, me, partner)
    for d in range(1, chips):
        greet(None, me, (y + d) % chips * CORES + c)
    expected = cols - 1 + chips + jnp.where(up, 1, 0) + jnp.where(down, 1, 0)
    locals_ = []

    def fetch(src, dst):
        copy = pltpu.make_async_copy(src, dst, local_sem.at[len(locals_)])
        copy.start()
        locals_.append(copy)

    fetch(win_refs[0], wq.at[me])
    at = 0
    for ref in win_refs[1:-1]:
        w = ref.shape[1]
        fetch(ref, wkv.at[me, :, pl.ds(at, w)])
        at += w
    fetch(win_refs[-1], wp.at[me])
    fetch(tok, tokv)
    fetch(gain_in, gain)
    fetch(wout_refs[0], wa.at[me])
    fetch(wout_refs[1], wb.at[me])
    fetch(pgain_in, pgain)
    fetch(sink_in, sink)
    with jax.named_scope("barrier"):
        pl.semaphore_wait(barrier, expected)

    class Sends:
        def __init__(self, whole):
            self.whole, self.conds = whole, []
            self.sem = send_sem.at[len(groups)]
            groups.append(self)

        def go(self, cond, src, dst, recv, dev):
            copy = pltpu.make_async_remote_copy(
                src_ref=src, dst_ref=dst, send_sem=self.sem, recv_sem=recv,
                device_id=dev, device_id_type=MESH,
            )
            when(cond, copy.start)
            self.conds.append((cond, copy))

        def wait(self):
            if self.whole is None:
                for cond, copy in self.conds:
                    when(cond, copy.wait_send)
                return
            sent = sum(1 if c is None else jnp.where(c, 1, 0) for c, _ in self.conds)
            for n in range(1, min(len(self.conds), self.whole.shape[0]) + 1):
                pl.when(sent == n)(functools.partial(self.wait_all, self.whole.at[pl.ds(0, n)]))

        def wait_all(self, ref=None):
            ref = self.whole if ref is None else ref
            if self.conds:
                pltpu.make_async_remote_copy(
                    src_ref=ref, dst_ref=ref, send_sem=self.sem, recv_sem=send_sem.at[0],
                    device_id=(me, partner), device_id_type=MESH,
                ).wait_send()

    groups = []

    def arrived(cond, dst, recv):
        copy = pltpu.make_async_remote_copy(
            src_ref=dst, dst_ref=dst, send_sem=send_sem.at[0], recv_sem=recv,
            device_id=(me, partner), device_id_type=MESH,
        )
        when(cond, copy.wait_recv)

    def at_distance(h):
        if h == 0:
            return ((z, None, None, None),)
        return (
            (z - h, z - h >= 0, up, me + cols),
            (z + h, z + h < levels, down, me - cols),
        )

    class Spread:
        def __init__(
            self, name, buf, sem, share=0.0, side_sem=None, ends=False, next_too=False
        ):
            self.name, self.buf, self.sem, self.side_sem = name, buf, sem, side_sem
            k = buf.shape[1]
            self.side = int(k * share) // 16 * 16 if cols > 1 and levels > 1 else 0
            self.k, self.ends, self.next_too = k, ends, next_too and cols > 1 and last > 1
            self.have, self.have_at_ends = set(), set()
            self.along_z, self.along_x = Sends(buf), Sends(buf)
            self.part_z = self.part_x = None
            if 0 < self.side < k:
                self.part_z = Sends(buf.at[:, pl.ds(0, self.side), :])
                self.part_x = Sends(buf.at[:, pl.ds(self.side, k - self.side), :])

        def piece(self, s, lo, hi):
            return self.buf.at[s] if (lo, hi) == (0, self.k) else self.buf.at[s, pl.ds(lo, hi - lo), :]

        def side_at(self, h):
            return self.side if h == (last if self.ends else 1) else 0

        def side_sems(self):
            return self.sem if self.side == self.k else self.side_sem

        def go(self, cond, s, lo, hi, sem, dev_sp, over_x=False):
            ref = self.piece(s, lo, hi)
            whole = (lo, hi) == (0, self.k)
            if over_x:
                sends = self.along_x if whole else self.part_x
            else:
                sends = self.along_z if whole else self.part_z
            sends.go(cond, ref, ref, sem.at[s], (dev_sp, t))

        def across(self, cond, s, lo=0):
            if lo == self.k:
                return
            for d in range(1, cols):
                self.go(cond, s, lo, self.k, self.sem, z * cols + (x + d) % cols, True)

        def begin_up(self, cond=None):
            self.go(both(up, cond), me, 0, self.k, self.sem, me + cols)

        def begin_down(self):
            self.go(down, me, 0, self.k, self.sem, me - cols)

        def begin_x(self, cond=None):
            self.across(cond, me)

        def forward(self, h, cond=None):
            with jax.named_scope(f"f{self.name}{h}"):
                for level, there, on, to in at_distance(h):
                    there = both(there, cond)
                    s = level * cols + x
                    arrived(there, self.buf.at[s], self.sem.at[s])
                    self.go(both(there, on), s, 0, self.k, self.sem, to)
                    if self.next_too and h == 1:
                        there = both(there, jnp.logical_and(level != 0, level != last))
                    self.across(there, s, self.side_at(h))

        def peers(self, level):
            return [level * cols + (x + cols - d) % cols for d in range(1, cols)]

        def forward_side(self, cond=None):
            if not self.side:
                return
            if not self.ends:
                self.take(0)
            sem = self.side_sems()
            for s in self.peers(z):
                if not self.ends:
                    self.go(up, s, 0, self.side, sem, me + cols)
                    self.go(down, s, 0, self.side, sem, me - cols)
                    continue
                self.go(cond, s, 0, self.side, sem, (last - z) * cols + x)

        def forward_next(self):
            if not self.next_too:
                return
            self.take(0, at_end)
            for s in self.peers(z):
                self.go(z == 0, s, 0, self.k, self.sem, me + cols)
                self.go(z == last, s, 0, self.k, self.sem, me - cols)

        def take(self, h, cond=None):
            if h in self.have or (h in self.have_at_ends and cond is at_end):
                return
            if cond is at_end:
                self.have_at_ends.add(h)
            else:
                self.have.add(h)
                cond = inner if h in self.have_at_ends else cond
            side = self.side_at(h)
            with jax.named_scope(f"t{self.name}{h}"):
                for level, there, _, _ in at_distance(h):
                    there = both(there, cond)
                    for s in self.peers(level):
                        if side:
                            arrived(there, self.piece(s, 0, side), self.side_sems().at[s])
                        if side < self.k:
                            arrived(there, self.piece(s, side, self.k), self.sem.at[s])

    spread_q = Spread("q", wq, sem_q, next_too=True)
    spread_kv = Spread("k", wkv, sem_kv, next_too=True)
    spread_p = Spread("p", wp, sem_p, 1.0)
    spread_a = Spread("a", wa, sem_a, SIDE_SHARE, sem_a_side, True, True)
    spread_b = Spread("b", wb, sem_b, 1.0, None, True, True)
    for copy in locals_[:n_in]:
        copy.wait()
    for spread in (spread_q, spread_kv, spread_p):
        spread.begin_up()
        spread.begin_down()
        spread.begin_x()
    locals_[n_in].wait()
    locals_[n_in + 1].wait()

    mine = pl.ds(pl.multiple_of(t * rows, rows), rows)
    wide = tokv[...].astype(F32)
    inverse = lax.rsqrt(jnp.mean(wide * wide, axis=1, keepdims=True) + EPS)
    piece = xs.shape[2]
    for i in range(n_sp):
        span = slice(i * piece, (i + 1) * piece)
        xs[i, mine, :] = (tokv[:, span].astype(F32) * inverse * gain[:, span]).astype(BF16)

    def rows_of(device):
        return xs.at[:, pl.ds(pl.multiple_of(device * rows, rows), rows), :]

    tokens_out = Sends(xs.at[:, pl.ds(0, (2 * chips - 1) * rows), :])
    for d in range(1, chips):
        tokens_out.go(
            None, rows_of(t), rows_of(t), sem_tok.at[t], (me, (y + d) % chips * CORES + c)
        )
    tokens_out.go(None, rows_of(t), rows_of(t), sem_tok.at[t], (me, partner))

    def chip_rows(chip):
        return pl.ds(pl.multiple_of(chip * per, per), per)

    near = [y]
    far = [(y + d) % chips for d in range(1, chips)]

    def project(spread, at, h, which):
        spread.take(h)
        w = spread.buf.shape[2]
        with jax.named_scope(f"m{spread.name}{h}"):
            for level, there, _, _ in at_distance(h):

                def run(level=level):
                    for chip in which:
                        r = chip_rows(chip)
                        value = None
                        for i in range(cols):
                            s = level * cols + i
                            part = jnp.dot(
                                xs[s, r, :], spread.buf[s], preferred_element_type=F32
                            )
                            value = part if value is None else value + part
                        if h == 0:
                            acc[r, at : at + w] = value
                        else:
                            acc[r, at : at + w] += value

                when(there, run)

    def project_q(h, which):
        project(spread_q, 0, h, which)

    def project_kv(h, which):
        project(spread_kv, qw, h, which)

    def project_p(h, which):
        project(spread_p, channel0, h, which)

    arrived(None, rows_of(partner), sem_tok.at[partner])
    for copy in locals_[n_in + 2 :]:
        copy.wait()

    def gather_tokens():
        with jax.named_scope("tokf"):
            for d in range(1, chips):
                at = (y + chips - d) % chips * CORES + c
                arrived(None, rows_of(at), sem_tok.at[at])
                tokens_out.go(None, rows_of(at), rows_of(at), sem_tok.at[at], (me, partner))

    def take_tokens():
        with jax.named_scope("tokt"):
            for d in range(1, chips):
                at = (y + chips - d) % chips * CORES + (1 - c)
                arrived(None, rows_of(at), sem_tok.at[at])

    for h in range(1, last):
        spread_q.forward(h)
        if h > 1:
            project_p(h - 2, near)
        spread_kv.forward(h)
        if h == 1:
            spread_q.forward_next()
        project_q(h - 1, near)
        spread_p.forward(h)
        if h == 1:
            spread_kv.forward_next()
        project_kv(h - 1, near)
    spread_p.forward_side()
    spread_a.begin_down()
    spread_a.begin_up()
    spread_b.begin_down()
    spread_b.begin_up(at_end)
    gather_tokens()
    done = max(0, last - 1)
    if last:
        spread_q.forward(last)
    take_tokens()
    for h in range(done):
        project_q(h, far)
        project_kv(h, far)
    for h in range(max(0, last - 2)):
        project_p(h, far)
    if last:
        spread_kv.forward(last)
    for h in range(done, last):
        project_q(h, near + far)
        project_kv(h, near + far)
    if last:
        spread_p.forward(last)
    for h in range(max(0, last - 2), last):
        if h != 1:
            project_p(h, near + far)
    project_q(last, far + near)
    if last:
        project_p(1, far + near)
    project_kv(last, far + near)

    def settle(lo, hi):
        for chip in range(chips):
            r = slice(chip * per, (chip + 1) * per)
            ext[WINDOW + chip * per : WINDOW + (chip + 1) * per, lo:hi] = acc[r, lo:hi].astype(BF16)

    with jax.named_scope("settleq"):
        settle(0, channel0)

    halo_out, tot_out = [Sends(None), Sends(None)], Sends(tot)

    def pass_on(cond, at, width, n, i):
        head = ext.at[pl.ds(WINDOW - n, n), pl.ds(at, width)]
        tail = ext.at[pl.ds(seq + WINDOW - n, n), pl.ds(at, width)]
        halo_out[i].go(both(cond, later), tail, head, sem_halo.at[i], (me + 1, t))
        return head

    head_kv = pass_on(None, qw, kw + vw, WINDOW, 0)

    group = t * pw // POOL_CH
    whole_prefix = group == POOL_GROUPS - 1
    halos = [
        (group == g, -(-(reach - 1) // 16) * 16)
        for g, reach in enumerate(SHORT_REACHES + (WINDOW,))
    ]

    def finish_pool_rows(cond):
        def run():
            with jax.named_scope("settlep"):
                settle(channel0, ext.shape[1])
                for n in range(blocks):
                    r = slice(WINDOW + n * WINDOW, 2 * WINDOW + n * WINDOW)
                    total = jnp.sum(ext[r, channel0:].astype(F32), axis=0, keepdims=True)
                    if n + 1 < blocks:
                        carry[n + 1] = jnp.broadcast_to(
                            total if n == 0 else carry[n, 0:1, :] + total, carry.shape[1:]
                        )
                    else:
                        tot[me] = jnp.broadcast_to(
                            total if n == 0 else carry[n, 0:1, :] + total, tot.shape[1:]
                        )
                carry[0] = jnp.zeros(carry.shape[1:], F32)

        when(cond, run)
        for is_group, n in halos:
            pass_on(both(is_group, cond), channel0, pw, n, 1)
        for d in range(1, n_sp):
            tot_out.go(
                both(both(whole_prefix, cond), me + d < n_sp), tot.at[me], tot.at[me],
                sem_tot.at[0], (me + d, t),
            )

    finish_pool_rows(inner)
    spread_a.begin_x()
    spread_b.begin_x(inner)
    spread_b.begin_up(inner)
    if last:
        spread_a.forward(1, inner)

    group_heads = qw // kw
    stacked = group_heads * WINDOW
    scale = HEAD_DIM ** (-0.5)

    def attend(n):
        q_rows = pl.ds(pl.multiple_of(n * WINDOW + WINDOW, WINDOW), WINDOW)
        k_rows = pl.ds(pl.multiple_of(n * WINDOW, WINDOW), 2 * WINDOW)
        queries = ext[q_rows, :qw]
        keys = ext[k_rows, qw : qw + kw]
        values = ext[k_rows, qw + kw : channel0]
        row = lax.broadcasted_iota(jnp.int32, (stacked, 2 * WINDOW), 0)
        q_index = row % WINDOW
        k_index = lax.broadcasted_iota(jnp.int32, (stacked, 2 * WINDOW), 1)
        lowest = jnp.where(me * blocks + n == 0, WINDOW, 0)
        allowed = (k_index > q_index) & (k_index <= q_index + WINDOW) & (k_index >= lowest)
        which = lax.broadcasted_iota(jnp.int32, (stacked, 1), 0) // WINDOW
        done = []
        for j in range(kw // HEAD_DIM):
            part = slice(j * HEAD_DIM, (j + 1) * HEAD_DIM)
            first = j * group_heads
            q = jnp.concatenate(
                [
                    queries[:, (first + g) * HEAD_DIM : (first + g + 1) * HEAD_DIM]
                    for g in range(group_heads)
                ],
                axis=0,
            )
            scores = (
                lax.dot_general(
                    q, keys[:, part], (((1,), (1,)), ((), ())), preferred_element_type=F32
                )
                * scale
            )
            scores = jnp.where(allowed, scores, -jnp.inf)
            sinks = jnp.full((stacked, 1), sink[first], F32)
            for g in range(1, group_heads):
                sinks = jnp.where(which == g, sink[first + g], sinks)
            peak = jnp.maximum(jnp.max(scores, axis=1, keepdims=True), sinks)
            expo = jnp.exp(scores - peak)
            denom = jnp.sum(expo, axis=1, keepdims=True) + jnp.exp(sinks - peak)
            probs = (expo * (1.0 / denom)).astype(BF16)
            got = jnp.dot(probs, values[:, part], preferred_element_type=F32)
            done += [got[g * WINDOW : (g + 1) * WINDOW] for g in range(group_heads)]
        to = pl.ds(pl.multiple_of(n * WINDOW, WINDOW), WINDOW)
        mix[to, :qw] = jnp.concatenate(done, axis=1).astype(BF16)

    if per % WINDOW == 0:
        span = per // WINDOW
        far_blocks, near_blocks = [chip * span for chip in far], [y * span]
    else:
        span = blocks
        far_blocks, near_blocks = [0], []

    def attend_later_blocks(firsts):
        with jax.named_scope("att"):
            for first in firsts:
                pl.loop(1, span)(lambda i, first=first: attend(first + i))

    def attend_first_block(firsts):
        with jax.named_scope("att0"):
            for first in firsts:
                cond = earlier if isinstance(first, int) else both(earlier, first == 0)
                arrived(cond, head_kv, sem_halo.at[0])
                attend(first)

    reach = jnp.where(
        group == 0, SHORT_REACHES[0], jnp.where(group == 1, SHORT_REACHES[1], WINDOW)
    )
    reach = jnp.where(whole_prefix, n_sp * seq, reach)
    lowest = jnp.where(whole_prefix, WINDOW, 0)

    def pool(firsts):
        with jax.named_scope("pool"):
            for first in firsts:

                @pl.loop(0, span)
                def _(i, first=first):
                    n = first + i
                    q_index = lax.broadcasted_iota(jnp.int32, (WINDOW, 2 * WINDOW), 0)
                    k_index = lax.broadcasted_iota(jnp.int32, (WINDOW, 2 * WINDOW), 1)
                    distance = q_index + WINDOW - k_index
                    band = (distance >= 0) & (distance < reach) & (k_index >= lowest)
                    band = jnp.where(band, 1.0, 0.0).astype(BF16)
                    k_rows = pl.ds(pl.multiple_of(n * WINDOW, WINDOW), 2 * WINDOW)
                    both_blocks = ext[k_rows, channel0:]
                    before = jnp.where(whole_prefix, carry[n, 0:1, :] + given[0:1, :], 0.0)
                    sums = jnp.dot(band, both_blocks, preferred_element_type=F32) + before
                    position = (
                        me * seq + n * WINDOW + lax.broadcasted_iota(jnp.int32, (WINDOW, 1), 0)
                    )
                    counted = jnp.minimum(position + 1, reach).astype(F32)
                    mixed = (sums / counted - both_blocks[WINDOW:].astype(F32)) * pgain[...]
                    to = pl.ds(pl.multiple_of(n * WINDOW, WINDOW), WINDOW)
                    mix[to, qw:] = mixed.astype(BF16)

    attend_later_blocks(far_blocks)
    if last >= 2:
        project_p(last, far + near)
    finish_pool_rows(at_end)
    spread_b.begin_x(at_end)
    if last:
        spread_a.forward(1, at_end)
        spread_b.forward(1, inner)
    attend_first_block(far_blocks)
    if last:
        spread_b.forward(1, at_end)
    spread_a.forward_next()
    with jax.named_scope("halopool"):
        for cond, n in halos:
            head = ext.at[pl.ds(WINDOW - n, n), pl.ds(channel0, pw)]
            arrived(both(cond, earlier), head, sem_halo.at[1])
        given[...] = jnp.zeros(given.shape, F32)
        for n in range(1, n_sp):

            def add(n=n):
                arrived(None, tot.at[pl.ds(0, n)], sem_tot.at[0])
                given[...] = jnp.sum(tot[:n], axis=0)

            when(both(whole_prefix, me == n), add)
    pool(far_blocks)

    def product(s, chip, core):
        r = pl.ds(pl.multiple_of((chip * CORES + core) * rows, rows), rows)
        return jnp.dot(mix[r, :qw], wa[s], preferred_element_type=F32) + jnp.dot(
            mix[r, qw:], wb[s], preferred_element_type=F32
        )

    def column(h):
        return [(there, level * cols + x) for level, there, _, _ in at_distance(h)]

    def others(h):
        return [
            (there, s)
            for level, there, _, _ in at_distance(h)
            for s in spread_a.peers(level)
        ]

    far_out, near_out, y_out = Sends(dfar), Sends(dnear), Sends(ysend)

    def multiply_far(pieces):
        for cond, s in pieces if chips > 1 else ():

            def give(s=s):
                for i, chip in enumerate(far):
                    dfar[s, i] = product(s, chip, 1 - c).astype(BF16)

            def keep(s=s):
                for i, chip in enumerate(far):
                    ofar[s, i] = product(s, chip, c)

            with jax.named_scope("mulf"):
                when(cond, give)
                far_out.go(cond, dfar.at[s], rfar.at[s], sem_far.at[s], (me, partner))
                when(cond, keep)

    def multiply_near(pieces):
        for cond, s in pieces:

            def give_near(s=s):
                dnear[s] = product(s, y, 1 - c).astype(BF16)

            def keep_near(s=s):
                onear[s] = product(s, y, c)

            with jax.named_scope("muln"):
                when(cond, give_near)
                near_out.go(cond, dnear.at[s], rnear.at[s], sem_near.at[0], (me, partner))
                when(cond, keep_near)

    def finish(pieces):
        for cond, s in pieces if chips > 1 else ():

            def pack(s=s):
                for i in range(chips - 1):
                    ysend[s, i] = (ofar[s, i] + rfar[s, i].astype(F32)).astype(BF16)

            with jax.named_scope("fin"):
                arrived(cond, rfar.at[s], sem_far.at[s])
                when(cond, pack)
                for i, chip in enumerate(far):
                    y_out.go(
                        cond, ysend.at[s, i], yrecv.at[s, i], sem_y.at[s, i],
                        (me, chip * CORES + c),
                    )

    def multiply(pieces):
        for piece in pieces:
            multiply_far([piece])
            multiply_near([piece])
            finish([piece])

    first = column(0)
    second = column(1) if last else []
    third = others(0)
    multiply_far(first)
    multiply_far(second)
    finish(first)
    if last >= 2:
        spread_a.forward(2)
        spread_b.forward(2, inner)
    finish(second)
    attend_later_blocks(near_blocks)
    spread_b.forward_next()
    attend_first_block(near_blocks)
    if last >= 2:
        spread_b.forward(2, at_end)
    spread_a.take(0)
    spread_b.take(0)
    spread_b.forward_side(z == last)
    spread_a.forward_side(z == last)
    multiply_far(third)
    pool(near_blocks)
    finish(third)
    fourth = column(2) if last >= 2 else []
    multiply_far(fourth)
    multiply_near(first)
    finish(fourth)

    def only(cond, pieces):
        return [(both(there, cond), s) for there, s in pieces]

    order = first + second + third + fourth

    def take_others(h, cond):
        spread_a.take(h, cond)
        spread_b.take(h, cond)
        multiply(only(cond, others(h)))
        order.extend(only(cond, others(h)))

    if last > 1:
        take_others(1, at_end)
    if last >= 3:
        spread_a.forward(3)
    spread_b.forward_side(z == 0)
    spread_a.forward_side(z == 0)
    multiply_near(second)
    if last >= 3:
        spread_b.forward(3)
    left = third + fourth
    for h in range(3, last + 1):
        multiply_far(column(h))
        multiply_near(left[:1])
        finish(column(h))
        left = left[1:] + column(h)
        order += column(h)
    for h in range(2, last):
        spread_a.take(h)
        spread_b.take(h)
        multiply_far(others(h))
        multiply_near(left[:2])
        finish(others(h))
        left = left[2:] + others(h)
        order += others(h)
    multiply_near(left)
    if last > 1:
        take_others(1, inner)
    if last:
        take_others(last, None)

    with jax.named_scope("wsend"):
        for sends in groups:
            if sends is tokens_out:
                sends.wait_all()
            elif sends not in (far_out, near_out, y_out):
                sends.wait()
    with jax.named_scope("final"):
        arrived(None, rnear, sem_near.at[0])
        w = wa.shape[2]
        for cond, s in order:

            def end(s=s):
                value = onear[s] + rnear[s].astype(F32)
                for i in range(chips - 1):
                    arrived(None, yrecv.at[s, i], sem_y.at[s, i])
                    value += yrecv[s, i].astype(F32)
                out[:, pl.ds(pl.multiple_of(s * w, w), w)] = value.astype(BF16)

            when(cond, end)

    for sends in (far_out, near_out, y_out):
        sends.wait_all()


def local(
    n_sp, n_tp, tokens_in, norm_gain, query_weight, key_weight, value_weight, pool_weight,
    sink_logit, pool_gain, attention_out_weight, pool_out_weight,
):
    rows, depth = tokens_in.shape
    seq = rows * n_tp
    ins = [query_weight, key_weight, value_weight, pool_weight]
    outs = [attention_out_weight, pool_out_weight]
    widths = tuple(w.shape[1] for w in ins)
    if widths[1] % 128:
        ins = [ins[0], jnp.concatenate(ins[1:3], axis=1), ins[3]]
    cols = math.gcd(n_sp, max(1, n_tp // CORES))
    chips = n_tp // CORES
    k_in, out_cols = ins[0].shape[0], outs[0].shape[1]
    width, others = sum(widths), max(1, chips - 1)
    qw, kw, vw, pw = widths
    vmem = pl.BlockSpec(memory_space=pltpu.VMEM)
    hbm = pl.BlockSpec(memory_space=pl.ANY)
    dma = pltpu.SemaphoreType.DMA
    return pl.pallas_call(
        functools.partial(kernel, n_sp, n_tp, cols, len(ins), len(outs), widths),
        out_shape=pltpu.VMEM((rows, depth), BF16),
        in_specs=[hbm] * (4 + len(ins) + len(outs)),
        out_specs=vmem,
        scratch_shapes=[
            pltpu.VMEM((rows, depth), BF16),
            pltpu.VMEM((n_sp, seq, depth // n_sp), BF16),
            pltpu.VMEM((n_sp, k_in, qw), BF16),
            pltpu.VMEM((n_sp, k_in, kw + vw), BF16),
            pltpu.VMEM((n_sp, k_in, pw), BF16),
            pltpu.VMEM((n_sp, outs[0].shape[0], out_cols), BF16),
            pltpu.VMEM((n_sp, outs[1].shape[0], out_cols), BF16),
            pltpu.VMEM((seq, width), F32),
            pltpu.VMEM((seq + WINDOW, width), BF16),
            pltpu.VMEM((seq, qw + pw), BF16),
            pltpu.VMEM((n_sp, 8, pw), F32),
            pltpu.VMEM((seq // WINDOW, 8, pw), F32),
            pltpu.VMEM((8, pw), F32),
            pltpu.VMEM((n_sp, others, rows, out_cols), BF16),
            pltpu.VMEM((n_sp, others, rows, out_cols), BF16),
            pltpu.VMEM((n_sp, rows, out_cols), BF16),
            pltpu.VMEM((n_sp, rows, out_cols), BF16),
            pltpu.VMEM((n_sp, others, rows, out_cols), BF16),
            pltpu.VMEM((n_sp, others, rows, out_cols), BF16),
            pltpu.VMEM((n_sp, others, rows, out_cols), F32),
            pltpu.VMEM((n_sp, rows, out_cols), F32),
            pltpu.VMEM((1, depth), F32),
            pltpu.VMEM((1, pw), F32),
            pltpu.SMEM(sink_logit.shape, F32),
            dma((len(ins) + len(outs) + 4,)),
            dma((SEND_GROUPS,)),
            dma((n_sp,)),
            dma((n_sp,)),
            dma((n_sp,)),
            dma((n_sp,)),
            dma((n_sp,)),
            dma((n_sp,)),
            dma((n_tp,)),
            dma((2,)),
            dma((1,)),
            dma((n_sp,)),
            dma((1,)),
            dma((n_sp, others)),
        ],
        compiler_params=pltpu.CompilerParams(
            collective_id=0, has_side_effects=True, vmem_limit_bytes=58 << 20
        ),
    )(
        tokens_in, norm_gain.reshape(1, -1), sink_logit, pool_gain.reshape(1, -1), *ins, *outs
    )


def solution(mesh):
    in_specs = (
        P(("sp", "tp"), None), P(), P("sp", "tp"), P("sp", "tp"), P("sp", "tp"), P("sp", "tp"),
        P("tp"), P("tp"), P("tp", "sp"), P("tp", "sp"),
    )
    out_specs = P(("sp", "tp"), None)
    return jax.shard_map(
        functools.partial(local, mesh.shape["sp"], mesh.shape["tp"]),
        mesh=mesh, in_specs=in_specs, out_specs=out_specs, check_vma=False,
    )
```

```python
import functools
import math

import jax
import jax.numpy as jnp
from jax import lax
from jax.experimental import pallas as pl
from jax.experimental.pallas import tpu as pltpu
from jax.sharding import PartitionSpec as P

HEAD_DIM = 64
POOL_CH = 256
POOL_GROUPS = 4
WINDOW = 128
EPS = 1e-06
SHORT_REACHES = (8, 32)
CORES = 2
SEND_GROUPS = 17
SIDE_SHARE = 0.375
MESH = pl.DeviceIdType.MESH
F32 = jnp.float32
BF16 = jnp.bfloat16


def when(cond, fn):
    if cond is None:
        fn()
    else:
        pl.when(cond)(fn)


def both(a, b):
    return b if a is None else (a if b is None else jnp.logical_and(a, b))


def layer(n_sp, n_tp, cols, n_in, n_out, widths, refs, late_sem, sem_near, sem_y):
    tok, gain_in, sink_in, pgain_in = refs[:4]
    win_refs = refs[4 : 4 + n_in]
    wout_refs = refs[4 + n_in : 4 + n_in + n_out]
    (
        out, tokv, xs, wq, wkv, wp, wa, wb, acc, ext, mix, tot, carry, given, dfar, rfar, dnear, rnear,
        ysend, yrecv, ofar, onear, gain, pgain, sink,
    ) = refs[4 + n_in + n_out :]
    qw, kw, vw, pw = widths
    levels = n_sp // cols
    chips = n_tp // CORES
    rows, seq = tok.shape[0], xs.shape[1]
    per = rows * CORES
    channel0 = qw + kw + vw
    blocks = seq // WINDOW
    me, t = lax.axis_index("sp"), lax.axis_index("tp")
    z, x = me // cols, me % cols
    y, c = t // CORES, t % CORES
    partner = y * CORES + (1 - c)
    up, down = z + 1 < levels, z > 0
    later, earlier = me + 1 < n_sp, me > 0
    last = levels - 1
    at_end = jnp.logical_or(z == 0, z == last)
    inner = jnp.logical_not(at_end)

    def arrived(cond, dst, recv):
        copy = pltpu.make_async_remote_copy(
            src_ref=dst, dst_ref=dst, send_sem=late_sem.at[0], recv_sem=recv,
            device_id=(me, partner), device_id_type=MESH,
        )
        when(cond, copy.wait_recv)

    def at_distance(h):
        if h == 0:
            return ((z, None, None, None),)
        return (
            (z - h, z - h >= 0, up, me + cols),
            (z + h, z + h < levels, down, me - cols),
        )

    def peers(level):
        return [level * cols + (x + cols - d) % cols for d in range(1, cols)]

    def column(h):
        return [(there, level * cols + x) for level, there, _, _ in at_distance(h)]

    def others(h):
        return [
            (there, s)
            for level, there, _, _ in at_distance(h)
            for s in peers(level)
        ]

    near = [y]
    far = [(y + d) % chips for d in range(1, chips)]

    def gather_and_multiply(
        local_sem, send_sem, sem_q, sem_kv, sem_p, sem_a, sem_b, sem_a_side, sem_tok, sem_halo,
        sem_tot, sem_far,
    ):
        ext[:WINDOW, qw:] = jnp.zeros((WINDOW, ext.shape[1] - qw), BF16)

        barrier = pltpu.get_barrier_semaphore()

        def greet(cond, sp, tp):
            when(
                cond,
                lambda: pl.semaphore_signal(
                    barrier, inc=1, device_id=(sp, tp), device_id_type=MESH
                ),
            )

        for d in range(1, cols):
            greet(None, z * cols + (x + d) % cols, t)
        greet(up, me + cols, t)
        greet(down, me - cols, t)
        greet(None, me, partner)
        for d in range(1, chips):
            greet(None, me, (y + d) % chips * CORES + c)
        expected = cols - 1 + chips + jnp.where(up, 1, 0) + jnp.where(down, 1, 0)

        locals_ = []

        def fetch(src, dst):
            copy = pltpu.make_async_copy(src, dst, local_sem.at[len(locals_)])
            copy.start()
            locals_.append(copy)

        fetch(win_refs[0], wq.at[me])
        at = 0
        for ref in win_refs[1:-1]:
            w = ref.shape[1]
            fetch(ref, wkv.at[me, :, pl.ds(at, w)])
            at += w
        fetch(win_refs[-1], wp.at[me])
        fetch(tok, tokv)
        fetch(gain_in, gain)
        fetch(wout_refs[0], wa.at[me])
        fetch(wout_refs[1], wb.at[me])
        fetch(pgain_in, pgain)
        fetch(sink_in, sink)
        pl.semaphore_wait(barrier, expected)

        class Sends:
            def __init__(self, whole, sem=None):
                self.whole, self.conds, self.sem = whole, [], sem
                if sem is None:
                    self.sem = send_sem.at[len(groups)]
                    groups.append(self)

            def go(self, cond, src, dst, recv, dev):
                copy = pltpu.make_async_remote_copy(
                    src_ref=src, dst_ref=dst, send_sem=self.sem, recv_sem=recv,
                    device_id=dev, device_id_type=MESH,
                )
                when(cond, copy.start)
                self.conds.append((cond, copy))

            def wait(self):
                if self.whole is None:
                    for cond, copy in self.conds:
                        when(cond, copy.wait_send)
                    return
                sent = sum(1 if c is None else jnp.where(c, 1, 0) for c, _ in self.conds)
                for n in range(1, min(len(self.conds), self.whole.shape[0]) + 1):
                    pl.when(sent == n)(functools.partial(self.wait_all, self.whole.at[pl.ds(0, n)]))

            def wait_all(self, ref=None):
                ref = self.whole if ref is None else ref
                if self.conds:
                    pltpu.make_async_remote_copy(
                        src_ref=ref, dst_ref=ref, send_sem=self.sem, recv_sem=send_sem.at[0],
                        device_id=(me, partner), device_id_type=MESH,
                    ).wait_send()

        groups = []

        class Spread:
            def __init__(
                self, name, buf, sem, share=0.0, side_sem=None, ends=False, next_too=False
            ):
                self.name, self.buf, self.sem, self.side_sem = name, buf, sem, side_sem
                k = buf.shape[1]
                self.side = int(k * share) // 16 * 16 if cols > 1 and levels > 1 else 0
                self.k, self.ends, self.next_too = k, ends, next_too and cols > 1 and last > 1
                self.have, self.have_at_ends = set(), set()
                self.along_z, self.along_x = Sends(buf), Sends(buf)
                self.part_z = self.part_x = None
                if 0 < self.side < k:
                    self.part_z = Sends(buf.at[:, pl.ds(0, self.side), :])
                    self.part_x = Sends(buf.at[:, pl.ds(self.side, k - self.side), :])

            def piece(self, s, lo, hi):
                return self.buf.at[s] if (lo, hi) == (0, self.k) else self.buf.at[s, pl.ds(lo, hi - lo), :]

            def side_at(self, h):
                return self.side if h == (last if self.ends else 1) else 0

            def side_sems(self):
                return self.sem if self.side == self.k else self.side_sem

            def go(self, cond, s, lo, hi, sem, dev_sp, over_x=False):
                ref = self.piece(s, lo, hi)
                whole = (lo, hi) == (0, self.k)
                if over_x:
                    sends = self.along_x if whole else self.part_x
                else:
                    sends = self.along_z if whole else self.part_z
                sends.go(cond, ref, ref, sem.at[s], (dev_sp, t))

            def across(self, cond, s, lo=0):
                if lo == self.k:
                    return
                for d in range(1, cols):
                    self.go(cond, s, lo, self.k, self.sem, z * cols + (x + d) % cols, True)

            def begin_up(self, cond=None):
                self.go(both(up, cond), me, 0, self.k, self.sem, me + cols)

            def begin_down(self):
                self.go(down, me, 0, self.k, self.sem, me - cols)

            def begin_x(self, cond=None):
                self.across(cond, me)

            def forward(self, h, cond=None):
                for level, there, on, to in at_distance(h):
                    there = both(there, cond)
                    s = level * cols + x
                    arrived(there, self.buf.at[s], self.sem.at[s])
                    self.go(both(there, on), s, 0, self.k, self.sem, to)
                    if self.next_too and h == 1:
                        there = both(there, jnp.logical_and(level != 0, level != last))
                    self.across(there, s, self.side_at(h))

            def forward_side(self, cond=None):
                if not self.side:
                    return
                if not self.ends:
                    self.take(0)
                sem = self.side_sems()
                for s in peers(z):
                    if not self.ends:
                        self.go(up, s, 0, self.side, sem, me + cols)
                        self.go(down, s, 0, self.side, sem, me - cols)
                        continue
                    self.go(cond, s, 0, self.side, sem, (last - z) * cols + x)

            def forward_next(self):
                if not self.next_too:
                    return
                self.take(0, at_end)
                for s in peers(z):
                    self.go(z == 0, s, 0, self.k, self.sem, me + cols)
                    self.go(z == last, s, 0, self.k, self.sem, me - cols)

            def take(self, h, cond=None):
                if h in self.have or (h in self.have_at_ends and cond is at_end):
                    return
                if cond is at_end:
                    self.have_at_ends.add(h)
                else:
                    self.have.add(h)
                    cond = inner if h in self.have_at_ends else cond
                side = self.side_at(h)
                for level, there, _, _ in at_distance(h):
                    there = both(there, cond)
                    for s in peers(level):
                        if side:
                            arrived(there, self.piece(s, 0, side), self.side_sems().at[s])
                        if side < self.k:
                            arrived(there, self.piece(s, side, self.k), self.sem.at[s])

        spread_q = Spread("q", wq, sem_q, next_too=True)
        spread_kv = Spread("k", wkv, sem_kv, next_too=True)
        spread_p = Spread("p", wp, sem_p, 1.0)
        spread_a = Spread("a", wa, sem_a, SIDE_SHARE, sem_a_side, True, True)
        spread_b = Spread("b", wb, sem_b, 1.0, None, True, True)
        for copy in locals_[:n_in]:
            copy.wait()
        for spread in (spread_q, spread_kv, spread_p):
            spread.begin_up()
            spread.begin_down()
            spread.begin_x()
        locals_[n_in].wait()
        locals_[n_in + 1].wait()

        mine = pl.ds(pl.multiple_of(t * rows, rows), rows)
        wide = tokv[...].astype(F32)
        inverse = lax.rsqrt(jnp.mean(wide * wide, axis=1, keepdims=True) + EPS)
        piece = xs.shape[2]
        for i in range(n_sp):
            span = slice(i * piece, (i + 1) * piece)
            xs[i, mine, :] = (tokv[:, span].astype(F32) * inverse * gain[:, span]).astype(BF16)

        def rows_of(device):
            return xs.at[:, pl.ds(pl.multiple_of(device * rows, rows), rows), :]

        tokens_out = Sends(xs.at[:, pl.ds(0, (2 * chips - 1) * rows), :])
        for d in range(1, chips):
            tokens_out.go(
                None, rows_of(t), rows_of(t), sem_tok.at[t], (me, (y + d) % chips * CORES + c)
            )
        tokens_out.go(None, rows_of(t), rows_of(t), sem_tok.at[t], (me, partner))

        def chip_rows(chip):
            return pl.ds(pl.multiple_of(chip * per, per), per)

        def project(spread, at, h, which):
            spread.take(h)
            w = spread.buf.shape[2]
            for level, there, _, _ in at_distance(h):

                def run(level=level):
                    for chip in which:
                        r = chip_rows(chip)
                        value = None
                        for i in range(cols):
                            s = level * cols + i
                            part = jnp.dot(
                                xs[s, r, :], spread.buf[s], preferred_element_type=F32
                            )
                            value = part if value is None else value + part
                        if h == 0:
                            acc[r, at : at + w] = value
                        else:
                            acc[r, at : at + w] += value

                when(there, run)

        def project_q(h, which):
            project(spread_q, 0, h, which)

        def project_kv(h, which):
            project(spread_kv, qw, h, which)

        def project_p(h, which):
            project(spread_p, channel0, h, which)

        arrived(None, rows_of(partner), sem_tok.at[partner])
        for copy in locals_[n_in + 2 :]:
            copy.wait()

        def gather_tokens():
            for d in range(1, chips):
                at = (y + chips - d) % chips * CORES + c
                arrived(None, rows_of(at), sem_tok.at[at])
                tokens_out.go(None, rows_of(at), rows_of(at), sem_tok.at[at], (me, partner))

        def take_tokens():
            for d in range(1, chips):
                at = (y + chips - d) % chips * CORES + (1 - c)
                arrived(None, rows_of(at), sem_tok.at[at])

        for h in range(1, last):
            spread_q.forward(h)
            if h > 1:
                project_p(h - 2, near)
            spread_kv.forward(h)
            if h == 1:
                spread_q.forward_next()
            project_q(h - 1, near)
            spread_p.forward(h)
            if h == 1:
                spread_kv.forward_next()
            project_kv(h - 1, near)
        spread_p.forward_side()
        spread_a.begin_down()
        spread_a.begin_up()
        spread_b.begin_down()
        spread_b.begin_up(at_end)
        gather_tokens()
        done = max(0, last - 1)
        if last:
            spread_q.forward(last)
        take_tokens()
        for h in range(done):
            project_q(h, far)
            project_kv(h, far)
        for h in range(max(0, last - 2)):
            project_p(h, far)
        if last:
            spread_kv.forward(last)
        for h in range(done, last):
            project_q(h, near + far)
            project_kv(h, near + far)
        if last:
            spread_p.forward(last)
        for h in range(max(0, last - 2), last):
            if h != 1:
                project_p(h, near + far)
        project_q(last, far + near)
        if last:
            project_p(1, far + near)
        project_kv(last, far + near)

        def settle(lo, hi):
            for chip in range(chips):
                r = slice(chip * per, (chip + 1) * per)
                ext[WINDOW + chip * per : WINDOW + (chip + 1) * per, lo:hi] = acc[r, lo:hi].astype(BF16)

        settle(0, channel0)

        halo_out, tot_out = [Sends(None), Sends(None)], Sends(tot)

        def pass_on(cond, at, width, n, i):
            head = ext.at[pl.ds(WINDOW - n, n), pl.ds(at, width)]
            tail = ext.at[pl.ds(seq + WINDOW - n, n), pl.ds(at, width)]
            halo_out[i].go(both(cond, later), tail, head, sem_halo.at[i], (me + 1, t))
            return head

        head_kv = pass_on(None, qw, kw + vw, WINDOW, 0)

        group = t * pw // POOL_CH
        whole_prefix = group == POOL_GROUPS - 1
        halos = [
            (group == g, -(-(reach - 1) // 16) * 16)
            for g, reach in enumerate(SHORT_REACHES + (WINDOW,))
        ]

        def finish_pool_rows(cond):
            def run():
                settle(channel0, ext.shape[1])
                for n in range(blocks):
                    r = slice(WINDOW + n * WINDOW, 2 * WINDOW + n * WINDOW)
                    total = jnp.sum(ext[r, channel0:].astype(F32), axis=0, keepdims=True)
                    if n + 1 < blocks:
                        carry[n + 1] = jnp.broadcast_to(
                            total if n == 0 else carry[n, 0:1, :] + total, carry.shape[1:]
                        )
                    else:
                        tot[me] = jnp.broadcast_to(
                            total if n == 0 else carry[n, 0:1, :] + total, tot.shape[1:]
                        )
                carry[0] = jnp.zeros(carry.shape[1:], F32)

            when(cond, run)
            for is_group, n in halos:
                pass_on(both(is_group, cond), channel0, pw, n, 1)
            for d in range(1, n_sp):
                tot_out.go(
                    both(both(whole_prefix, cond), me + d < n_sp), tot.at[me], tot.at[me],
                    sem_tot.at[0], (me + d, t),
                )

        finish_pool_rows(inner)
        spread_a.begin_x()
        spread_b.begin_x(inner)
        spread_b.begin_up(inner)
        if last:
            spread_a.forward(1, inner)

        group_heads = qw // kw
        stacked = group_heads * WINDOW
        scale = HEAD_DIM ** (-0.5)

        def attend(n):
            q_rows = pl.ds(pl.multiple_of(n * WINDOW + WINDOW, WINDOW), WINDOW)
            k_rows = pl.ds(pl.multiple_of(n * WINDOW, WINDOW), 2 * WINDOW)
            queries = ext[q_rows, :qw]
            keys = ext[k_rows, qw : qw + kw]
            values = ext[k_rows, qw + kw : channel0]
            row = lax.broadcasted_iota(jnp.int32, (stacked, 2 * WINDOW), 0)
            q_index = row % WINDOW
            k_index = lax.broadcasted_iota(jnp.int32, (stacked, 2 * WINDOW), 1)
            lowest = jnp.where(me * blocks + n == 0, WINDOW, 0)
            allowed = (k_index > q_index) & (k_index <= q_index + WINDOW) & (k_index >= lowest)
            which = lax.broadcasted_iota(jnp.int32, (stacked, 1), 0) // WINDOW
            done = []
            for j in range(kw // HEAD_DIM):
                part = slice(j * HEAD_DIM, (j + 1) * HEAD_DIM)
                first = j * group_heads
                q = jnp.concatenate(
                    [
                        queries[:, (first + g) * HEAD_DIM : (first + g + 1) * HEAD_DIM]
                        for g in range(group_heads)
                    ],
                    axis=0,
                )
                scores = (
                    lax.dot_general(
                        q, keys[:, part], (((1,), (1,)), ((), ())), preferred_element_type=F32
                    )
                    * scale
                )
                scores = jnp.where(allowed, scores, -jnp.inf)
                sinks = jnp.full((stacked, 1), sink[first], F32)
                for g in range(1, group_heads):
                    sinks = jnp.where(which == g, sink[first + g], sinks)
                peak = jnp.maximum(jnp.max(scores, axis=1, keepdims=True), sinks)
                expo = jnp.exp(scores - peak)
                denom = jnp.sum(expo, axis=1, keepdims=True) + jnp.exp(sinks - peak)
                probs = (expo * (1.0 / denom)).astype(BF16)
                got = jnp.dot(probs, values[:, part], preferred_element_type=F32)
                done += [got[g * WINDOW : (g + 1) * WINDOW] for g in range(group_heads)]
            to = pl.ds(pl.multiple_of(n * WINDOW, WINDOW), WINDOW)
            mix[to, :qw] = jnp.concatenate(done, axis=1).astype(BF16)

        if per % WINDOW == 0:
            span = per // WINDOW
            far_blocks, near_blocks = [chip * span for chip in far], [y * span]
        else:
            span = blocks
            far_blocks, near_blocks = [0], []

        def attend_later_blocks(firsts):
            for first in firsts:
                pl.loop(1, span)(lambda i, first=first: attend(first + i))

        def attend_first_block(firsts):
            for first in firsts:
                cond = earlier if isinstance(first, int) else both(earlier, first == 0)
                arrived(cond, head_kv, sem_halo.at[0])
                attend(first)

        reach = jnp.where(
            group == 0, SHORT_REACHES[0], jnp.where(group == 1, SHORT_REACHES[1], WINDOW)
        )
        reach = jnp.where(whole_prefix, n_sp * seq, reach)
        lowest = jnp.where(whole_prefix, WINDOW, 0)

        def pool(firsts):
            for first in firsts:

                @pl.loop(0, span)
                def _(i, first=first):
                    n = first + i
                    q_index = lax.broadcasted_iota(jnp.int32, (WINDOW, 2 * WINDOW), 0)
                    k_index = lax.broadcasted_iota(jnp.int32, (WINDOW, 2 * WINDOW), 1)
                    distance = q_index + WINDOW - k_index
                    band = (distance >= 0) & (distance < reach) & (k_index >= lowest)
                    band = jnp.where(band, 1.0, 0.0).astype(BF16)
                    k_rows = pl.ds(pl.multiple_of(n * WINDOW, WINDOW), 2 * WINDOW)
                    both_blocks = ext[k_rows, channel0:]
                    before = jnp.where(whole_prefix, carry[n, 0:1, :] + given[0:1, :], 0.0)
                    sums = jnp.dot(band, both_blocks, preferred_element_type=F32) + before
                    position = (
                        me * seq + n * WINDOW + lax.broadcasted_iota(jnp.int32, (WINDOW, 1), 0)
                    )
                    counted = jnp.minimum(position + 1, reach).astype(F32)
                    mixed = (sums / counted - both_blocks[WINDOW:].astype(F32)) * pgain[...]
                    to = pl.ds(pl.multiple_of(n * WINDOW, WINDOW), WINDOW)
                    mix[to, qw:] = mixed.astype(BF16)

        attend_later_blocks(far_blocks)
        if last >= 2:
            project_p(last, far + near)
        finish_pool_rows(at_end)
        spread_b.begin_x(at_end)
        if last:
            spread_a.forward(1, at_end)
            spread_b.forward(1, inner)
        attend_first_block(far_blocks)
        if last:
            spread_b.forward(1, at_end)
        spread_a.forward_next()
        for cond, n in halos:
            head = ext.at[pl.ds(WINDOW - n, n), pl.ds(channel0, pw)]
            arrived(both(cond, earlier), head, sem_halo.at[1])
        given[...] = jnp.zeros(given.shape, F32)
        for n in range(1, n_sp):

            def add(n=n):
                arrived(None, tot.at[pl.ds(0, n)], sem_tot.at[0])
                given[...] = jnp.sum(tot[:n], axis=0)

            when(both(whole_prefix, me == n), add)
        pool(far_blocks)

        def product(s, chip, core):
            r = pl.ds(pl.multiple_of((chip * CORES + core) * rows, rows), rows)
            return jnp.dot(mix[r, :qw], wa[s], preferred_element_type=F32) + jnp.dot(
                mix[r, qw:], wb[s], preferred_element_type=F32
            )

        far_out = Sends(dfar)
        near_out, y_out = Sends(dnear, late_sem.at[0]), Sends(ysend, late_sem.at[1])

        def multiply_far(pieces):
            for cond, s in pieces if chips > 1 else ():

                def give(s=s):
                    for i, chip in enumerate(far):
                        dfar[s, i] = product(s, chip, 1 - c).astype(BF16)

                def keep(s=s):
                    for i, chip in enumerate(far):
                        ofar[s, i] = product(s, chip, c)

                when(cond, give)
                far_out.go(cond, dfar.at[s], rfar.at[s], sem_far.at[s], (me, partner))
                when(cond, keep)

        def multiply_near(pieces):
            for cond, s in pieces:

                def give_near(s=s):
                    dnear[s] = product(s, y, 1 - c).astype(BF16)

                def keep_near(s=s):
                    onear[s] = product(s, y, c)

                when(cond, give_near)
                near_out.go(cond, dnear.at[s], rnear.at[s], sem_near.at[0], (me, partner))
                when(cond, keep_near)

        def finish(pieces):
            for cond, s in pieces if chips > 1 else ():

                def pack(s=s):
                    for i in range(chips - 1):
                        ysend[s, i] = (ofar[s, i] + rfar[s, i].astype(F32)).astype(BF16)

                arrived(cond, rfar.at[s], sem_far.at[s])
                when(cond, pack)
                for i, chip in enumerate(far):
                    y_out.go(
                        cond, ysend.at[s, i], yrecv.at[s, i], sem_y.at[s, i],
                        (me, chip * CORES + c),
                    )

        def multiply(pieces):
            for piece in pieces:
                multiply_far([piece])
                multiply_near([piece])
                finish([piece])

        first = column(0)
        second = column(1) if last else []
        third = others(0)
        multiply_far(first)
        multiply_far(second)
        finish(first)
        if last >= 2:
            spread_a.forward(2)
            spread_b.forward(2, inner)
        finish(second)
        attend_later_blocks(near_blocks)
        spread_b.forward_next()
        attend_first_block(near_blocks)
        if last >= 2:
            spread_b.forward(2, at_end)
        spread_a.take(0)
        spread_b.take(0)
        spread_b.forward_side(z == last)
        spread_a.forward_side(z == last)
        multiply_far(third)
        pool(near_blocks)
        finish(third)
        fourth = column(2) if last >= 2 else []
        multiply_far(fourth)
        multiply_near(first)
        finish(fourth)

        def only(cond, pieces):
            return [(both(there, cond), s) for there, s in pieces]


        def take_others(h, cond):
            spread_a.take(h, cond)
            spread_b.take(h, cond)
            multiply(only(cond, others(h)))

        if last > 1:
            take_others(1, at_end)
        if last >= 3:
            spread_a.forward(3)
        spread_b.forward_side(z == 0)
        spread_a.forward_side(z == 0)
        multiply_near(second)
        if last >= 3:
            spread_b.forward(3)
        left = third + fourth
        for h in range(3, last + 1):
            multiply_far(column(h))
            multiply_near(left[:1])
            finish(column(h))
            left = left[1:] + column(h)
        for h in range(2, last):
            spread_a.take(h)
            spread_b.take(h)
            multiply_far(others(h))
            multiply_near(left[:2])
            finish(others(h))
            left = left[2:] + others(h)
        multiply_near(left)
        if last > 1:
            take_others(1, inner)
        if last:
            take_others(last, None)

        for sends in groups:
            if sends is tokens_out:
                sends.wait_all()
            elif sends is far_out:
                sends.wait_all()
            else:
                sends.wait()
    dma = pltpu.SemaphoreType.DMA
    per_shard = dma((n_sp,))
    pl.run_scoped(
        gather_and_multiply, dma((n_in + n_out + 4,)), dma((SEND_GROUPS,)), per_shard, per_shard,
        per_shard, per_shard, per_shard, per_shard, dma((n_tp,)), dma((2,)), dma((1,)), per_shard,
    )

    order = column(0)
    if last:
        order = order + column(1)
    order = order + others(0)
    for h in range(2, last + 1):
        order = order + column(h)
    for h in range(1, last + 1):
        order = order + others(h)

    arrived(None, rnear, sem_near.at[0])
    w = wa.shape[2]
    for cond, s in order:

        def end(s=s):
            value = onear[s] + rnear[s].astype(F32)
            for i in range(chips - 1):
                arrived(None, yrecv.at[s, i], sem_y.at[s, i])
                value += yrecv[s, i].astype(F32)
            out[:, pl.ds(pl.multiple_of(s * w, w), w)] = value.astype(BF16)

        when(cond, end)

    for ref, i in ((dnear, 0), (ysend, 1)) if chips > 1 else ((dnear, 0),):
        pltpu.make_async_remote_copy(
            src_ref=ref, dst_ref=ref, send_sem=late_sem.at[i], recv_sem=sem_near.at[0],
            device_id=(me, partner), device_id_type=MESH,
        ).wait_send()


def kernel(n_sp, n_tp, cols, n_in, n_out, widths, *refs):
    dma = pltpu.SemaphoreType.DMA
    others = max(1, n_tp // CORES - 1)
    pl.run_scoped(
        functools.partial(layer, n_sp, n_tp, cols, n_in, n_out, widths, refs),
        dma((2,)), dma((1,)), dma((n_sp, others)),
    )


def local(
    n_sp, n_tp, tokens_in, norm_gain, query_weight, key_weight, value_weight, pool_weight,
    sink_logit, pool_gain, attention_out_weight, pool_out_weight,
):
    rows, depth = tokens_in.shape
    seq = rows * n_tp
    ins = [query_weight, key_weight, value_weight, pool_weight]
    outs = [attention_out_weight, pool_out_weight]
    widths = tuple(w.shape[1] for w in ins)
    if widths[1] % 128:
        ins = [ins[0], jnp.concatenate(ins[1:3], axis=1), ins[3]]
    cols = math.gcd(n_sp, max(1, n_tp // CORES))
    chips = n_tp // CORES
    k_in, out_cols = ins[0].shape[0], outs[0].shape[1]
    width, others = sum(widths), max(1, chips - 1)
    qw, kw, vw, pw = widths
    vmem = pl.BlockSpec(memory_space=pltpu.VMEM)
    hbm = pl.BlockSpec(memory_space=pl.ANY)
    return pl.pallas_call(
        functools.partial(kernel, n_sp, n_tp, cols, len(ins), len(outs), widths),
        out_shape=pltpu.VMEM((rows, depth), BF16),
        in_specs=[hbm] * (4 + len(ins) + len(outs)),
        out_specs=vmem,
        scratch_shapes=[
            pltpu.VMEM((rows, depth), BF16),
            pltpu.VMEM((n_sp, seq, depth // n_sp), BF16),
            pltpu.VMEM((n_sp, k_in, qw), BF16),
            pltpu.VMEM((n_sp, k_in, kw + vw), BF16),
            pltpu.VMEM((n_sp, k_in, pw), BF16),
            pltpu.VMEM((n_sp, outs[0].shape[0], out_cols), BF16),
            pltpu.VMEM((n_sp, outs[1].shape[0], out_cols), BF16),
            pltpu.VMEM((seq, width), F32),
            pltpu.VMEM((seq + WINDOW, width), BF16),
            pltpu.VMEM((seq, qw + pw), BF16),
            pltpu.VMEM((n_sp, 8, pw), F32),
            pltpu.VMEM((seq // WINDOW, 8, pw), F32),
            pltpu.VMEM((8, pw), F32),
            pltpu.VMEM((n_sp, others, rows, out_cols), BF16),
            pltpu.VMEM((n_sp, others, rows, out_cols), BF16),
            pltpu.VMEM((n_sp, rows, out_cols), BF16),
            pltpu.VMEM((n_sp, rows, out_cols), BF16),
            pltpu.VMEM((n_sp, others, rows, out_cols), BF16),
            pltpu.VMEM((n_sp, others, rows, out_cols), BF16),
            pltpu.VMEM((n_sp, others, rows, out_cols), F32),
            pltpu.VMEM((n_sp, rows, out_cols), F32),
            pltpu.VMEM((1, depth), F32),
            pltpu.VMEM((1, pw), F32),
            pltpu.SMEM(sink_logit.shape, F32),
        ],
        compiler_params=pltpu.CompilerParams(
            collective_id=0, has_side_effects=True, vmem_limit_bytes=58 << 20
        ),
    )(
        tokens_in, norm_gain.reshape(1, -1), sink_logit, pool_gain.reshape(1, -1), *ins, *outs
    )


def solution(mesh):
    in_specs = (
        P(("sp", "tp"), None), P(), P("sp", "tp"), P("sp", "tp"), P("sp", "tp"), P("sp", "tp"),
        P("tp"), P("tp"), P("tp", "sp"), P("tp", "sp"),
    )
    out_specs = P(("sp", "tp"), None)
    return jax.shard_map(
        functools.partial(local, mesh.shape["sp"], mesh.shape["tp"]),
        mesh=mesh, in_specs=in_specs, out_specs=out_specs, check_vma=False,
    )
```

```python
import functools
import math

import jax
import jax.numpy as jnp
from jax import lax
from jax.experimental import pallas as pl
from jax.experimental.pallas import tpu as pltpu
from jax.sharding import PartitionSpec as P

HEAD_DIM = 64
POOL_CH = 256
POOL_GROUPS = 4
WINDOW = 128
EPS = 1e-06
SHORT_REACHES = (8, 32)
CORES = 2
SEND_GROUPS = 17
SIDE_SHARE = 0.375
MESH = pl.DeviceIdType.MESH
F32 = jnp.float32
BF16 = jnp.bfloat16


def when(cond, fn):
    if cond is None:
        fn()
    else:
        pl.when(cond)(fn)


def both(a, b):
    return b if a is None else (a if b is None else jnp.logical_and(a, b))


def layer(n_sp, n_tp, cols, n_in, n_out, widths, refs, late_sem, sem_near, sem_y):
    tok, gain_in, sink_in, pgain_in = refs[:4]
    win_refs = refs[4 : 4 + n_in]
    wout_refs = refs[4 + n_in : 4 + n_in + n_out]
    (
        out, tokv, xs, wq, wkv, wp, wa, wb, acc, ext, mix, tot, carry, given, dfar, rfar, dnear, rnear,
        ysend, yrecv, ofar, onear, gain, pgain, sink,
    ) = refs[4 + n_in + n_out :]
    qw, kw, vw, pw = widths
    levels = n_sp // cols
    chips = n_tp // CORES
    rows, seq = tok.shape[0], xs.shape[1]
    per = rows * CORES
    channel0 = qw + kw + vw
    blocks = seq // WINDOW
    me, t = lax.axis_index("sp"), lax.axis_index("tp")
    z, x = me // cols, me % cols
    y, c = t // CORES, t % CORES
    partner = y * CORES + (1 - c)
    up, down = z + 1 < levels, z > 0
    later, earlier = me + 1 < n_sp, me > 0
    last = levels - 1
    at_end = jnp.logical_or(z == 0, z == last)
    inner = jnp.logical_not(at_end)

    def arrived(cond, dst, recv):
        copy = pltpu.make_async_remote_copy(
            src_ref=dst, dst_ref=dst, send_sem=late_sem.at[0], recv_sem=recv,
            device_id=(me, partner), device_id_type=MESH,
        )
        when(cond, copy.wait_recv)

    def at_distance(h):
        if h == 0:
            return ((z, None, None, None),)
        return (
            (z - h, z - h >= 0, up, me + cols),
            (z + h, z + h < levels, down, me - cols),
        )

    def peers(level):
        return [level * cols + (x + cols - d) % cols for d in range(1, cols)]

    def column(h):
        return [(there, level * cols + x) for level, there, _, _ in at_distance(h)]

    def others(h):
        return [
            (there, s)
            for level, there, _, _ in at_distance(h)
            for s in peers(level)
        ]

    near = [y]
    far = [(y + d) % chips for d in range(1, chips)]

    def gather_and_multiply(
        local_sem, send_sem, sem_q, sem_kv, sem_p, sem_a, sem_b, sem_a_side, sem_tok, sem_halo,
        sem_tot, sem_far,
    ):
        ext[:WINDOW, qw:] = jnp.zeros((WINDOW, ext.shape[1] - qw), BF16)

        barrier = pltpu.get_barrier_semaphore()

        def greet(cond, sp, tp):
            when(
                cond,
                lambda: pl.semaphore_signal(
                    barrier, inc=1, device_id=(sp, tp), device_id_type=MESH
                ),
            )

        for d in range(1, cols):
            greet(None, z * cols + (x + d) % cols, t)
        greet(up, me + cols, t)
        greet(down, me - cols, t)
        greet(None, me, partner)
        for d in range(1, chips):
            greet(None, me, (y + d) % chips * CORES + c)
        expected = cols - 1 + chips + jnp.where(up, 1, 0) + jnp.where(down, 1, 0)

        locals_ = []

        def fetch(src, dst):
            copy = pltpu.make_async_copy(src, dst, local_sem.at[len(locals_)])
            copy.start()
            locals_.append(copy)

        fetch(win_refs[0], wq.at[me])
        at = 0
        for ref in win_refs[1:-1]:
            w = ref.shape[1]
            fetch(ref, wkv.at[me, :, pl.ds(at, w)])
            at += w
        fetch(win_refs[-1], wp.at[me])
        fetch(tok, tokv)
        fetch(gain_in, gain)
        fetch(wout_refs[0], wa.at[me])
        fetch(wout_refs[1], wb.at[me])
        fetch(pgain_in, pgain)
        fetch(sink_in, sink)
        pl.semaphore_wait(barrier, expected)

        class Sends:
            def __init__(self, whole, sem=None):
                self.whole, self.conds, self.sem = whole, [], sem
                if sem is None:
                    self.sem = send_sem.at[len(groups)]
                    groups.append(self)

            def go(self, cond, src, dst, recv, dev):
                copy = pltpu.make_async_remote_copy(
                    src_ref=src, dst_ref=dst, send_sem=self.sem, recv_sem=recv,
                    device_id=dev, device_id_type=MESH,
                )
                when(cond, copy.start)
                self.conds.append((cond, copy))

            def wait(self):
                if self.whole is None:
                    for cond, copy in self.conds:
                        when(cond, copy.wait_send)
                    return
                sent = sum(1 if c is None else jnp.where(c, 1, 0) for c, _ in self.conds)
                for n in range(1, min(len(self.conds), self.whole.shape[0]) + 1):
                    pl.when(sent == n)(functools.partial(self.wait_all, self.whole.at[pl.ds(0, n)]))

            def wait_all(self, ref=None):
                ref = self.whole if ref is None else ref
                if self.conds:
                    pltpu.make_async_remote_copy(
                        src_ref=ref, dst_ref=ref, send_sem=self.sem, recv_sem=send_sem.at[0],
                        device_id=(me, partner), device_id_type=MESH,
                    ).wait_send()

        groups = []

        class Spread:
            def __init__(
                self, name, buf, sem, share=0.0, side_sem=None, ends=False, next_too=False
            ):
                self.name, self.buf, self.sem, self.side_sem = name, buf, sem, side_sem
                k = buf.shape[1]
                self.side = int(k * share) // 16 * 16 if cols > 1 and levels > 1 else 0
                self.k, self.ends, self.next_too = k, ends, next_too and cols > 1 and last > 1
                self.have, self.have_at_ends = set(), set()
                self.along_z, self.along_x = Sends(buf), Sends(buf)
                self.part_z = self.part_x = None
                if 0 < self.side < k:
                    self.part_z = Sends(buf.at[:, pl.ds(0, self.side), :])
                    self.part_x = Sends(buf.at[:, pl.ds(self.side, k - self.side), :])

            def piece(self, s, lo, hi):
                return self.buf.at[s] if (lo, hi) == (0, self.k) else self.buf.at[s, pl.ds(lo, hi - lo), :]

            def side_at(self, h):
                return self.side if h == (last if self.ends else 1) else 0

            def side_sems(self):
                return self.sem if self.side == self.k else self.side_sem

            def go(self, cond, s, lo, hi, sem, dev_sp, over_x=False):
                ref = self.piece(s, lo, hi)
                whole = (lo, hi) == (0, self.k)
                if over_x:
                    sends = self.along_x if whole else self.part_x
                else:
                    sends = self.along_z if whole else self.part_z
                sends.go(cond, ref, ref, sem.at[s], (dev_sp, t))

            def across(self, cond, s, lo=0):
                if lo == self.k:
                    return
                for d in range(1, cols):
                    self.go(cond, s, lo, self.k, self.sem, z * cols + (x + d) % cols, True)

            def begin_up(self, cond=None):
                self.go(both(up, cond), me, 0, self.k, self.sem, me + cols)

            def begin_down(self):
                self.go(down, me, 0, self.k, self.sem, me - cols)

            def begin_x(self, cond=None):
                self.across(cond, me)

            def forward(self, h, cond=None):
                for level, there, on, to in at_distance(h):
                    there = both(there, cond)
                    s = level * cols + x
                    arrived(there, self.buf.at[s], self.sem.at[s])
                    self.go(both(there, on), s, 0, self.k, self.sem, to)
                    if self.next_too and h == 1:
                        there = both(there, jnp.logical_and(level != 0, level != last))
                    self.across(there, s, self.side_at(h))

            def forward_side(self, cond=None):
                if not self.side:
                    return
                if not self.ends:
                    self.take(0)
                sem = self.side_sems()
                for s in peers(z):
                    if not self.ends:
                        self.go(up, s, 0, self.side, sem, me + cols)
                        self.go(down, s, 0, self.side, sem, me - cols)
                        continue
                    self.go(cond, s, 0, self.side, sem, (last - z) * cols + x)

            def forward_next(self):
                if not self.next_too:
                    return
                self.take(0, at_end)
                for s in peers(z):
                    self.go(z == 0, s, 0, self.k, self.sem, me + cols)
                    self.go(z == last, s, 0, self.k, self.sem, me - cols)

            def take(self, h, cond=None):
                if h in self.have or (h in self.have_at_ends and cond is at_end):
                    return
                if cond is at_end:
                    self.have_at_ends.add(h)
                else:
                    self.have.add(h)
                    cond = inner if h in self.have_at_ends else cond
                side = self.side_at(h)
                for level, there, _, _ in at_distance(h):
                    there = both(there, cond)
                    for s in peers(level):
                        if side:
                            arrived(there, self.piece(s, 0, side), self.side_sems().at[s])
                        if side < self.k:
                            arrived(there, self.piece(s, side, self.k), self.sem.at[s])

        spread_q = Spread("q", wq, sem_q, next_too=True)
        spread_kv = Spread("k", wkv, sem_kv, next_too=True)
        spread_p = Spread("p", wp, sem_p, 1.0)
        spread_a = Spread("a", wa, sem_a, SIDE_SHARE, sem_a_side, True, True)
        spread_b = Spread("b", wb, sem_b, 1.0, None, True, True)
        for copy in locals_[:n_in]:
            copy.wait()
        for spread in (spread_q, spread_kv, spread_p):
            spread.begin_up()
            spread.begin_down()
            spread.begin_x()
        locals_[n_in].wait()
        locals_[n_in + 1].wait()

        mine = pl.ds(pl.multiple_of(t * rows, rows), rows)
        wide = tokv[...].astype(F32)
        inverse = lax.rsqrt(jnp.mean(wide * wide, axis=1, keepdims=True) + EPS)
        piece = xs.shape[2]
        for i in range(n_sp):
            span = slice(i * piece, (i + 1) * piece)
            xs[i, mine, :] = (tokv[:, span].astype(F32) * inverse * gain[:, span]).astype(BF16)

        def rows_of(device):
            return xs.at[:, pl.ds(pl.multiple_of(device * rows, rows), rows), :]

        tokens_out = Sends(xs.at[:, pl.ds(0, (2 * chips - 1) * rows), :])
        for d in range(1, chips):
            tokens_out.go(
                None, rows_of(t), rows_of(t), sem_tok.at[t], (me, (y + d) % chips * CORES + c)
            )
        tokens_out.go(None, rows_of(t), rows_of(t), sem_tok.at[t], (me, partner))

        def chip_rows(chip):
            return pl.ds(pl.multiple_of(chip * per, per), per)

        def project(spread, at, h, which):
            spread.take(h)
            w = spread.buf.shape[2]
            for level, there, _, _ in at_distance(h):

                def run(level=level):
                    for chip in which:
                        r = chip_rows(chip)
                        value = None
                        for i in range(cols):
                            s = level * cols + i
                            part = jnp.dot(
                                xs[s, r, :], spread.buf[s], preferred_element_type=F32
                            )
                            value = part if value is None else value + part
                        if h == 0:
                            acc[r, at : at + w] = value
                        else:
                            acc[r, at : at + w] += value

                when(there, run)

        def project_q(h, which):
            project(spread_q, 0, h, which)

        def project_kv(h, which):
            project(spread_kv, qw, h, which)

        def project_p(h, which):
            project(spread_p, channel0, h, which)

        arrived(None, rows_of(partner), sem_tok.at[partner])
        for copy in locals_[n_in + 2 :]:
            copy.wait()

        def gather_tokens():
            for d in range(1, chips):
                at = (y + chips - d) % chips * CORES + c
                arrived(None, rows_of(at), sem_tok.at[at])
                tokens_out.go(None, rows_of(at), rows_of(at), sem_tok.at[at], (me, partner))

        def take_tokens():
            for d in range(1, chips):
                at = (y + chips - d) % chips * CORES + (1 - c)
                arrived(None, rows_of(at), sem_tok.at[at])

        for h in range(1, last):
            spread_q.forward(h)
            if h > 1:
                project_p(h - 2, near)
            spread_kv.forward(h)
            if h == 1:
                spread_q.forward_next()
            project_q(h - 1, near)
            spread_p.forward(h)
            if h == 1:
                spread_kv.forward_next()
            project_kv(h - 1, near)
        spread_p.forward_side()
        spread_a.begin_down()
        spread_a.begin_up()
        spread_b.begin_down()
        spread_b.begin_up(at_end)
        gather_tokens()
        done = max(0, last - 1)
        if last:
            spread_q.forward(last)
        take_tokens()
        for h in range(done):
            project_q(h, far)
            project_kv(h, far)
        for h in range(max(0, last - 2)):
            project_p(h, far)
        if last:
            spread_kv.forward(last)
        for h in range(done, last):
            project_q(h, near + far)
            project_kv(h, near + far)
        if last:
            spread_p.forward(last)
        for h in range(max(0, last - 2), last):
            if h != 1:
                project_p(h, near + far)
        project_q(last, far + near)
        if last:
            project_p(1, far + near)
        project_kv(last, far + near)

        def settle(lo, hi):
            for chip in range(chips):
                r = slice(chip * per, (chip + 1) * per)
                ext[WINDOW + chip * per : WINDOW + (chip + 1) * per, lo:hi] = acc[r, lo:hi].astype(BF16)

        settle(0, channel0)

        halo_out, tot_out = [Sends(None), Sends(None)], Sends(tot)

        def pass_on(cond, at, width, n, i):
            head = ext.at[pl.ds(WINDOW - n, n), pl.ds(at, width)]
            tail = ext.at[pl.ds(seq + WINDOW - n, n), pl.ds(at, width)]
            halo_out[i].go(both(cond, later), tail, head, sem_halo.at[i], (me + 1, t))
            return head

        head_kv = pass_on(None, qw, kw + vw, WINDOW, 0)

        group = t * pw // POOL_CH
        whole_prefix = group == POOL_GROUPS - 1
        halos = [
            (group == g, -(-(reach - 1) // 16) * 16)
            for g, reach in enumerate(SHORT_REACHES + (WINDOW,))
        ]

        def finish_pool_rows(cond):
            def run():
                settle(channel0, ext.shape[1])
                for n in range(blocks):
                    r = slice(WINDOW + n * WINDOW, 2 * WINDOW + n * WINDOW)
                    total = jnp.sum(ext[r, channel0:].astype(F32), axis=0, keepdims=True)
                    if n + 1 < blocks:
                        carry[n + 1] = jnp.broadcast_to(
                            total if n == 0 else carry[n, 0:1, :] + total, carry.shape[1:]
                        )
                    else:
                        tot[me] = jnp.broadcast_to(
                            total if n == 0 else carry[n, 0:1, :] + total, tot.shape[1:]
                        )
                carry[0] = jnp.zeros(carry.shape[1:], F32)

            when(cond, run)
            for is_group, n in halos:
                pass_on(both(is_group, cond), channel0, pw, n, 1)
            for d in range(1, n_sp):
                tot_out.go(
                    both(both(whole_prefix, cond), me + d < n_sp), tot.at[me], tot.at[me],
                    sem_tot.at[0], (me + d, t),
                )

        finish_pool_rows(inner)
        spread_a.begin_x()
        spread_b.begin_x(inner)
        spread_b.begin_up(inner)
        if last:
            spread_a.forward(1, inner)

        group_heads = qw // kw
        stacked = group_heads * WINDOW
        scale = HEAD_DIM ** (-0.5)

        def attend(n):
            q_rows = pl.ds(pl.multiple_of(n * WINDOW + WINDOW, WINDOW), WINDOW)
            k_rows = pl.ds(pl.multiple_of(n * WINDOW, WINDOW), 2 * WINDOW)
            queries = ext[q_rows, :qw]
            keys = ext[k_rows, qw : qw + kw]
            values = ext[k_rows, qw + kw : channel0]
            row = lax.broadcasted_iota(jnp.int32, (stacked, 2 * WINDOW), 0)
            q_index = row % WINDOW
            k_index = lax.broadcasted_iota(jnp.int32, (stacked, 2 * WINDOW), 1)
            lowest = jnp.where(me * blocks + n == 0, WINDOW, 0)
            allowed = (k_index > q_index) & (k_index <= q_index + WINDOW) & (k_index >= lowest)
            which = lax.broadcasted_iota(jnp.int32, (stacked, 1), 0) // WINDOW
            done = []
            for j in range(kw // HEAD_DIM):
                part = slice(j * HEAD_DIM, (j + 1) * HEAD_DIM)
                first = j * group_heads
                q = jnp.concatenate(
                    [
                        queries[:, (first + g) * HEAD_DIM : (first + g + 1) * HEAD_DIM]
                        for g in range(group_heads)
                    ],
                    axis=0,
                )
                scores = (
                    lax.dot_general(
                        q, keys[:, part], (((1,), (1,)), ((), ())), preferred_element_type=F32
                    )
                    * scale
                )
                scores = jnp.where(allowed, scores, -jnp.inf)
                sinks = jnp.full((stacked, 1), sink[first], F32)
                for g in range(1, group_heads):
                    sinks = jnp.where(which == g, sink[first + g], sinks)
                peak = jnp.maximum(jnp.max(scores, axis=1, keepdims=True), sinks)
                expo = jnp.exp(scores - peak)
                denom = jnp.sum(expo, axis=1, keepdims=True) + jnp.exp(sinks - peak)
                probs = (expo * (1.0 / denom)).astype(BF16)
                got = jnp.dot(probs, values[:, part], preferred_element_type=F32)
                done += [got[g * WINDOW : (g + 1) * WINDOW] for g in range(group_heads)]
            to = pl.ds(pl.multiple_of(n * WINDOW, WINDOW), WINDOW)
            mix[to, :qw] = jnp.concatenate(done, axis=1).astype(BF16)

        if per % WINDOW == 0:
            span = per // WINDOW
            far_blocks, near_blocks = [chip * span for chip in far], [y * span]
        else:
            span = blocks
            far_blocks, near_blocks = [0], []

        def attend_later_blocks(firsts):
            for first in firsts:
                pl.loop(1, span)(lambda i, first=first: attend(first + i))

        def attend_first_block(firsts):
            for first in firsts:
                cond = earlier if isinstance(first, int) else both(earlier, first == 0)
                arrived(cond, head_kv, sem_halo.at[0])
                attend(first)

        reach = jnp.where(
            group == 0, SHORT_REACHES[0], jnp.where(group == 1, SHORT_REACHES[1], WINDOW)
        )
        reach = jnp.where(whole_prefix, n_sp * seq, reach)
        lowest = jnp.where(whole_prefix, WINDOW, 0)

        def pool(firsts):
            for first in firsts:

                @pl.loop(0, span)
                def _(i, first=first):
                    n = first + i
                    q_index = lax.broadcasted_iota(jnp.int32, (WINDOW, 2 * WINDOW), 0)
                    k_index = lax.broadcasted_iota(jnp.int32, (WINDOW, 2 * WINDOW), 1)
                    distance = q_index + WINDOW - k_index
                    band = (distance >= 0) & (distance < reach) & (k_index >= lowest)
                    band = jnp.where(band, 1.0, 0.0).astype(BF16)
                    k_rows = pl.ds(pl.multiple_of(n * WINDOW, WINDOW), 2 * WINDOW)
                    both_blocks = ext[k_rows, channel0:]
                    before = jnp.where(whole_prefix, carry[n, 0:1, :] + given[0:1, :], 0.0)
                    sums = jnp.dot(band, both_blocks, preferred_element_type=F32) + before
                    position = (
                        me * seq + n * WINDOW + lax.broadcasted_iota(jnp.int32, (WINDOW, 1), 0)
                    )
                    counted = jnp.minimum(position + 1, reach).astype(F32)
                    mixed = (sums / counted - both_blocks[WINDOW:].astype(F32)) * pgain[...]
                    to = pl.ds(pl.multiple_of(n * WINDOW, WINDOW), WINDOW)
                    mix[to, qw:] = mixed.astype(BF16)

        attend_later_blocks(far_blocks)
        if last >= 2:
            project_p(last, far + near)
        finish_pool_rows(at_end)
        spread_b.begin_x(at_end)
        if last:
            spread_a.forward(1, at_end)
            spread_b.forward(1, inner)
        attend_first_block(far_blocks)
        if last:
            spread_b.forward(1, at_end)
        spread_a.forward_next()
        for cond, n in halos:
            head = ext.at[pl.ds(WINDOW - n, n), pl.ds(channel0, pw)]
            arrived(both(cond, earlier), head, sem_halo.at[1])
        given[...] = jnp.zeros(given.shape, F32)
        for n in range(1, n_sp):

            def add(n=n):
                arrived(None, tot.at[pl.ds(0, n)], sem_tot.at[0])
                given[...] = jnp.sum(tot[:n], axis=0)

            when(both(whole_prefix, me == n), add)
        pool(far_blocks)

        def product(s, chip, core):
            r = pl.ds(pl.multiple_of((chip * CORES + core) * rows, rows), rows)
            return jnp.dot(mix[r, :qw], wa[s], preferred_element_type=F32) + jnp.dot(
                mix[r, qw:], wb[s], preferred_element_type=F32
            )

        far_out = Sends(dfar)
        near_out, y_out = Sends(dnear, late_sem.at[0]), Sends(ysend, late_sem.at[1])

        def multiply_far(pieces):
            for cond, s in pieces if chips > 1 else ():

                def give(s=s):
                    for i, chip in enumerate(far):
                        dfar[s, i] = product(s, chip, 1 - c).astype(BF16)

                def keep(s=s):
                    for i, chip in enumerate(far):
                        ofar[s, i] = product(s, chip, c)

                when(cond, give)
                far_out.go(cond, dfar.at[s], rfar.at[s], sem_far.at[s], (me, partner))
                when(cond, keep)

        def multiply_near(pieces):
            for cond, s in pieces:

                def give_near(s=s):
                    dnear[s] = product(s, y, 1 - c).astype(BF16)

                def keep_near(s=s):
                    onear[s] = product(s, y, c)

                when(cond, give_near)
                near_out.go(cond, dnear.at[s], rnear.at[s], sem_near.at[0], (me, partner))
                when(cond, keep_near)

        def finish(pieces):
            for cond, s in pieces if chips > 1 else ():

                def pack(s=s):
                    for i in range(chips - 1):
                        ysend[s, i] = (ofar[s, i] + rfar[s, i].astype(F32)).astype(BF16)

                arrived(cond, rfar.at[s], sem_far.at[s])
                when(cond, pack)
                for i, chip in enumerate(far):
                    y_out.go(
                        cond, ysend.at[s, i], yrecv.at[s, i], sem_y.at[s, i],
                        (me, chip * CORES + c),
                    )

        def multiply(pieces):
            for piece in pieces:
                multiply_far([piece])
                multiply_near([piece])
                finish([piece])

        first = column(0)
        second = column(1) if last else []
        third = others(0)
        multiply_far(first)
        multiply_far(second)
        finish(first)
        if last >= 2:
            spread_a.forward(2)
            spread_b.forward(2, inner)
        finish(second)
        attend_later_blocks(near_blocks)
        spread_b.forward_next()
        spread_a.take(0)
        spread_b.take(0)
        multiply_far(third)
        attend_first_block(near_blocks)
        finish(third)
        if last >= 2:
            spread_b.forward(2, at_end)
        spread_b.forward_side(z == last)
        spread_a.forward_side(z == last)
        fourth = column(2) if last >= 2 else []
        multiply_far(fourth)
        pool(near_blocks)
        multiply_near(first)
        finish(fourth)

        def only(cond, pieces):
            return [(both(there, cond), s) for there, s in pieces]


        def take_others(h, cond):
            spread_a.take(h, cond)
            spread_b.take(h, cond)
            multiply(only(cond, others(h)))

        if last > 1:
            take_others(1, at_end)
        if last >= 3:
            spread_a.forward(3)
        spread_b.forward_side(z == 0)
        spread_a.forward_side(z == 0)
        if last >= 3:
            spread_b.forward(3)
        left = second + third + fourth
        for h in range(3, last + 1):
            multiply_far(column(h))
            multiply_near(left[:2])
            finish(column(h))
            left = left[2:] + column(h)
        for h in range(2, last):
            spread_a.take(h)
            spread_b.take(h)
            multiply_far(others(h))
            multiply_near(left[:2])
            finish(others(h))
            left = left[2:] + others(h)
        multiply_near(left)
        if last > 1:
            take_others(1, inner)
        if last:
            take_others(last, None)

        for sends in groups:
            if sends is tokens_out:
                sends.wait_all()
            elif sends is far_out:
                sends.wait_all()
            else:
                sends.wait()
    dma = pltpu.SemaphoreType.DMA
    per_shard = dma((n_sp,))
    pl.run_scoped(
        gather_and_multiply, dma((n_in + n_out + 4,)), dma((SEND_GROUPS,)), per_shard, per_shard,
        per_shard, per_shard, per_shard, per_shard, dma((n_tp,)), dma((2,)), dma((1,)), per_shard,
    )

    order = column(0)
    if last:
        order = order + column(1)
    order = order + others(0)
    for h in range(2, last + 1):
        order = order + column(h)
    for h in range(1, last + 1):
        order = order + others(h)

    arrived(None, rnear, sem_near.at[0])
    w = wa.shape[2]
    for cond, s in order:

        def end(s=s):
            value = onear[s] + rnear[s].astype(F32)
            for i in range(chips - 1):
                arrived(None, yrecv.at[s, i], sem_y.at[s, i])
                value += yrecv[s, i].astype(F32)
            out[:, pl.ds(pl.multiple_of(s * w, w), w)] = value.astype(BF16)

        when(cond, end)

    for ref, i in ((dnear, 0), (ysend, 1)) if chips > 1 else ((dnear, 0),):
        pltpu.make_async_remote_copy(
            src_ref=ref, dst_ref=ref, send_sem=late_sem.at[i], recv_sem=sem_near.at[0],
            device_id=(me, partner), device_id_type=MESH,
        ).wait_send()


def kernel(n_sp, n_tp, cols, n_in, n_out, widths, *refs):
    dma = pltpu.SemaphoreType.DMA
    others = max(1, n_tp // CORES - 1)
    pl.run_scoped(
        functools.partial(layer, n_sp, n_tp, cols, n_in, n_out, widths, refs),
        dma((2,)), dma((1,)), dma((n_sp, others)),
    )


def local(
    n_sp, n_tp, tokens_in, norm_gain, query_weight, key_weight, value_weight, pool_weight,
    sink_logit, pool_gain, attention_out_weight, pool_out_weight,
):
    rows, depth = tokens_in.shape
    seq = rows * n_tp
    ins = [query_weight, key_weight, value_weight, pool_weight]
    outs = [attention_out_weight, pool_out_weight]
    widths = tuple(w.shape[1] for w in ins)
    if widths[1] % 128:
        ins = [ins[0], jnp.concatenate(ins[1:3], axis=1), ins[3]]
    cols = math.gcd(n_sp, max(1, n_tp // CORES))
    chips = n_tp // CORES
    k_in, out_cols = ins[0].shape[0], outs[0].shape[1]
    width, others = sum(widths), max(1, chips - 1)
    qw, kw, vw, pw = widths
    vmem = pl.BlockSpec(memory_space=pltpu.VMEM)
    hbm = pl.BlockSpec(memory_space=pl.ANY)
    return pl.pallas_call(
        functools.partial(kernel, n_sp, n_tp, cols, len(ins), len(outs), widths),
        out_shape=pltpu.VMEM((rows, depth), BF16),
        in_specs=[hbm] * (4 + len(ins) + len(outs)),
        out_specs=vmem,
        scratch_shapes=[
            pltpu.VMEM((rows, depth), BF16),
            pltpu.VMEM((n_sp, seq, depth // n_sp), BF16),
            pltpu.VMEM((n_sp, k_in, qw), BF16),
            pltpu.VMEM((n_sp, k_in, kw + vw), BF16),
            pltpu.VMEM((n_sp, k_in, pw), BF16),
            pltpu.VMEM((n_sp, outs[0].shape[0], out_cols), BF16),
            pltpu.VMEM((n_sp, outs[1].shape[0], out_cols), BF16),
            pltpu.VMEM((seq, width), F32),
            pltpu.VMEM((seq + WINDOW, width), BF16),
            pltpu.VMEM((seq, qw + pw), BF16),
            pltpu.VMEM((n_sp, 8, pw), F32),
            pltpu.VMEM((seq // WINDOW, 8, pw), F32),
            pltpu.VMEM((8, pw), F32),
            pltpu.VMEM((n_sp, others, rows, out_cols), BF16),
            pltpu.VMEM((n_sp, others, rows, out_cols), BF16),
            pltpu.VMEM((n_sp, rows, out_cols), BF16),
            pltpu.VMEM((n_sp, rows, out_cols), BF16),
            pltpu.VMEM((n_sp, others, rows, out_cols), BF16),
            pltpu.VMEM((n_sp, others, rows, out_cols), BF16),
            pltpu.VMEM((n_sp, others, rows, out_cols), F32),
            pltpu.VMEM((n_sp, rows, out_cols), F32),
            pltpu.VMEM((1, depth), F32),
            pltpu.VMEM((1, pw), F32),
            pltpu.SMEM(sink_logit.shape, F32),
        ],
        compiler_params=pltpu.CompilerParams(
            collective_id=0, has_side_effects=True, vmem_limit_bytes=58 << 20
        ),
    )(
        tokens_in, norm_gain.reshape(1, -1), sink_logit, pool_gain.reshape(1, -1), *ins, *outs
    )


def solution(mesh):
    in_specs = (
        P(("sp", "tp"), None), P(), P("sp", "tp"), P("sp", "tp"), P("sp", "tp"), P("sp", "tp"),
        P("tp"), P("tp"), P("tp", "sp"), P("tp", "sp"),
    )
    out_specs = P(("sp", "tp"), None)
    return jax.shard_map(
        functools.partial(local, mesh.shape["sp"], mesh.shape["tp"]),
        mesh=mesh, in_specs=in_specs, out_specs=out_specs, check_vma=False,
    )
```

```python
import functools
import math

import jax
import jax.numpy as jnp
from jax import lax
from jax.experimental import pallas as pl
from jax.experimental.pallas import tpu as pltpu
from jax.sharding import PartitionSpec as P

HEAD_DIM = 64
POOL_CH = 256
POOL_GROUPS = 4
WINDOW = 128
EPS = 1e-06
SHORT_REACHES = (8, 32)
CORES = 2
SEND_GROUPS = 17
SIDE_SHARE = 0.375
MESH = pl.DeviceIdType.MESH
F32 = jnp.float32
BF16 = jnp.bfloat16


def when(cond, fn):
    if cond is None:
        fn()
    else:
        pl.when(cond)(fn)


def both(a, b):
    return b if a is None else (a if b is None else jnp.logical_and(a, b))


def layer(n_sp, n_tp, cols, n_in, n_out, widths, refs, late_sem, sem_near, sem_y):
    tok, gain_in, sink_in, pgain_in = refs[:4]
    win_refs = refs[4 : 4 + n_in]
    wout_refs = refs[4 + n_in : 4 + n_in + n_out]
    (
        out, tokv, xs, wq, wkv, wp, wa, wb, acc, ext, mix, tot, carry, given, dfar, rfar, dnear, rnear,
        ysend, yrecv, ofar, onear, gain, pgain, sink,
    ) = refs[4 + n_in + n_out :]
    qw, kw, vw, pw = widths
    levels = n_sp // cols
    chips = n_tp // CORES
    rows, seq = tok.shape[0], xs.shape[1]
    per = rows * CORES
    channel0 = qw + kw + vw
    blocks = seq // WINDOW
    me, t = lax.axis_index("sp"), lax.axis_index("tp")
    z, x = me // cols, me % cols
    y, c = t // CORES, t % CORES
    partner = y * CORES + (1 - c)
    up, down = z + 1 < levels, z > 0
    later, earlier = me + 1 < n_sp, me > 0
    last = levels - 1
    at_end = jnp.logical_or(z == 0, z == last)
    inner = jnp.logical_not(at_end)

    def arrived(cond, dst, recv):
        copy = pltpu.make_async_remote_copy(
            src_ref=dst, dst_ref=dst, send_sem=late_sem.at[0], recv_sem=recv,
            device_id=(me, partner), device_id_type=MESH,
        )
        when(cond, copy.wait_recv)

    def at_distance(h):
        if h == 0:
            return ((z, None, None, None),)
        return (
            (z - h, z - h >= 0, up, me + cols),
            (z + h, z + h < levels, down, me - cols),
        )

    def peers(level):
        return [level * cols + (x + cols - d) % cols for d in range(1, cols)]

    def column(h):
        return [(there, level * cols + x) for level, there, _, _ in at_distance(h)]

    def others(h):
        return [
            (there, s)
            for level, there, _, _ in at_distance(h)
            for s in peers(level)
        ]

    near = [y]
    far = [(y + d) % chips for d in range(1, chips)]

    def gather_and_multiply(
        local_sem, send_sem, sem_q, sem_kv, sem_p, sem_a, sem_b, sem_a_side, sem_tok, sem_halo,
        sem_tot, sem_far,
    ):
        ext[:WINDOW, qw:] = jnp.zeros((WINDOW, ext.shape[1] - qw), BF16)

        barrier = pltpu.get_barrier_semaphore()

        def greet(cond, sp, tp):
            when(
                cond,
                lambda: pl.semaphore_signal(
                    barrier, inc=1, device_id=(sp, tp), device_id_type=MESH
                ),
            )

        for d in range(1, cols):
            greet(None, z * cols + (x + d) % cols, t)
        greet(up, me + cols, t)
        greet(down, me - cols, t)
        greet(None, me, partner)
        for d in range(1, chips):
            greet(None, me, (y + d) % chips * CORES + c)
        expected = cols - 1 + chips + jnp.where(up, 1, 0) + jnp.where(down, 1, 0)

        locals_ = []

        def fetch(src, dst):
            copy = pltpu.make_async_copy(src, dst, local_sem.at[len(locals_)])
            copy.start()
            locals_.append(copy)

        fetch(win_refs[0], wq.at[me])
        at = 0
        for ref in win_refs[1:-1]:
            w = ref.shape[1]
            fetch(ref, wkv.at[me, :, pl.ds(at, w)])
            at += w
        fetch(win_refs[-1], wp.at[me])
        fetch(tok, tokv)
        fetch(gain_in, gain)
        fetch(wout_refs[0], wa.at[me])
        fetch(wout_refs[1], wb.at[me])
        fetch(pgain_in, pgain)
        fetch(sink_in, sink)
        pl.semaphore_wait(barrier, expected)

        class Sends:
            def __init__(self, whole, sem=None):
                self.whole, self.conds, self.sem = whole, [], sem
                if sem is None:
                    self.sem = send_sem.at[len(groups)]
                    groups.append(self)

            def go(self, cond, src, dst, recv, dev):
                copy = pltpu.make_async_remote_copy(
                    src_ref=src, dst_ref=dst, send_sem=self.sem, recv_sem=recv,
                    device_id=dev, device_id_type=MESH,
                )
                when(cond, copy.start)
                self.conds.append((cond, copy))

            def wait(self):
                if self.whole is None:
                    for cond, copy in self.conds:
                        when(cond, copy.wait_send)
                    return
                sent = sum(1 if c is None else jnp.where(c, 1, 0) for c, _ in self.conds)
                for n in range(1, min(len(self.conds), self.whole.shape[0]) + 1):
                    pl.when(sent == n)(functools.partial(self.wait_all, self.whole.at[pl.ds(0, n)]))

            def wait_all(self, ref=None):
                ref = self.whole if ref is None else ref
                if self.conds:
                    pltpu.make_async_remote_copy(
                        src_ref=ref, dst_ref=ref, send_sem=self.sem, recv_sem=send_sem.at[0],
                        device_id=(me, partner), device_id_type=MESH,
                    ).wait_send()

        groups = []

        class Spread:
            def __init__(
                self, name, buf, sem, share=0.0, side_sem=None, ends=False, next_too=False
            ):
                self.name, self.buf, self.sem, self.side_sem = name, buf, sem, side_sem
                k = buf.shape[1]
                self.side = int(k * share) // 16 * 16 if cols > 1 and levels > 1 else 0
                self.k, self.ends, self.next_too = k, ends, next_too and cols > 1 and last > 1
                self.have, self.have_at_ends = set(), set()
                self.along_z, self.along_x = Sends(buf), Sends(buf)
                self.part_z = self.part_x = None
                if 0 < self.side < k:
                    self.part_z = Sends(buf.at[:, pl.ds(0, self.side), :])
                    self.part_x = Sends(buf.at[:, pl.ds(self.side, k - self.side), :])

            def piece(self, s, lo, hi):
                return self.buf.at[s] if (lo, hi) == (0, self.k) else self.buf.at[s, pl.ds(lo, hi - lo), :]

            def side_at(self, h):
                return self.side if h == (last if self.ends else 1) else 0

            def side_sems(self):
                return self.sem if self.side == self.k else self.side_sem

            def go(self, cond, s, lo, hi, sem, dev_sp, over_x=False):
                ref = self.piece(s, lo, hi)
                whole = (lo, hi) == (0, self.k)
                if over_x:
                    sends = self.along_x if whole else self.part_x
                else:
                    sends = self.along_z if whole else self.part_z
                sends.go(cond, ref, ref, sem.at[s], (dev_sp, t))

            def across(self, cond, s, lo=0):
                if lo == self.k:
                    return
                for d in range(1, cols):
                    self.go(cond, s, lo, self.k, self.sem, z * cols + (x + d) % cols, True)

            def begin_up(self, cond=None):
                self.go(both(up, cond), me, 0, self.k, self.sem, me + cols)

            def begin_down(self):
                self.go(down, me, 0, self.k, self.sem, me - cols)

            def begin_x(self, cond=None):
                self.across(cond, me)

            def forward(self, h, cond=None):
                for level, there, on, to in at_distance(h):
                    there = both(there, cond)
                    s = level * cols + x
                    arrived(there, self.buf.at[s], self.sem.at[s])
                    self.go(both(there, on), s, 0, self.k, self.sem, to)
                    if self.next_too and h == 1:
                        there = both(there, jnp.logical_and(level != 0, level != last))
                    self.across(there, s, self.side_at(h))

            def forward_side(self, cond=None):
                if not self.side:
                    return
                if not self.ends:
                    self.take(0)
                sem = self.side_sems()
                for s in peers(z):
                    if not self.ends:
                        self.go(up, s, 0, self.side, sem, me + cols)
                        self.go(down, s, 0, self.side, sem, me - cols)
                        continue
                    self.go(cond, s, 0, self.side, sem, (last - z) * cols + x)

            def forward_next(self):
                if not self.next_too:
                    return
                self.take(0, at_end)
                for s in peers(z):
                    self.go(z == 0, s, 0, self.k, self.sem, me + cols)
                    self.go(z == last, s, 0, self.k, self.sem, me - cols)

            def take(self, h, cond=None):
                if h in self.have or (h in self.have_at_ends and cond is at_end):
                    return
                if cond is at_end:
                    self.have_at_ends.add(h)
                else:
                    self.have.add(h)
                    cond = inner if h in self.have_at_ends else cond
                side = self.side_at(h)
                for level, there, _, _ in at_distance(h):
                    there = both(there, cond)
                    for s in peers(level):
                        if side:
                            arrived(there, self.piece(s, 0, side), self.side_sems().at[s])
                        if side < self.k:
                            arrived(there, self.piece(s, side, self.k), self.sem.at[s])

        spread_q = Spread("q", wq, sem_q, next_too=True)
        spread_kv = Spread("k", wkv, sem_kv, next_too=True)
        spread_p = Spread("p", wp, sem_p, 1.0)
        spread_a = Spread("a", wa, sem_a, SIDE_SHARE, sem_a_side, True, True)
        spread_b = Spread("b", wb, sem_b, 1.0, None, True, True)
        for copy in locals_[:n_in]:
            copy.wait()
        for spread in (spread_q, spread_kv, spread_p):
            spread.begin_up()
            spread.begin_down()
            spread.begin_x()
        locals_[n_in].wait()
        locals_[n_in + 1].wait()

        mine = pl.ds(pl.multiple_of(t * rows, rows), rows)
        wide = tokv[...].astype(F32)
        inverse = lax.rsqrt(jnp.mean(wide * wide, axis=1, keepdims=True) + EPS)
        piece = xs.shape[2]
        for i in range(n_sp):
            span = slice(i * piece, (i + 1) * piece)
            xs[i, mine, :] = (tokv[:, span].astype(F32) * inverse * gain[:, span]).astype(BF16)

        def rows_of(device):
            return xs.at[:, pl.ds(pl.multiple_of(device * rows, rows), rows), :]

        tokens_out = Sends(xs.at[:, pl.ds(0, (2 * chips - 1) * rows), :])
        for d in range(1, chips):
            tokens_out.go(
                None, rows_of(t), rows_of(t), sem_tok.at[t], (me, (y + d) % chips * CORES + c)
            )
        tokens_out.go(None, rows_of(t), rows_of(t), sem_tok.at[t], (me, partner))

        def chip_rows(chip):
            return pl.ds(pl.multiple_of(chip * per, per), per)

        def project(spread, at, h, which):
            spread.take(h)
            w = spread.buf.shape[2]
            for level, there, _, _ in at_distance(h):

                def run(level=level):
                    for chip in which:
                        r = chip_rows(chip)
                        value = None
                        for i in range(cols):
                            s = level * cols + i
                            part = jnp.dot(
                                xs[s, r, :], spread.buf[s], preferred_element_type=F32
                            )
                            value = part if value is None else value + part
                        if h == 0:
                            acc[r, at : at + w] = value
                        else:
                            acc[r, at : at + w] += value

                when(there, run)

        def project_q(h, which):
            project(spread_q, 0, h, which)

        def project_kv(h, which):
            project(spread_kv, qw, h, which)

        def project_p(h, which):
            project(spread_p, channel0, h, which)

        arrived(None, rows_of(partner), sem_tok.at[partner])
        for copy in locals_[n_in + 2 :]:
            copy.wait()

        def gather_tokens():
            for d in range(1, chips):
                at = (y + chips - d) % chips * CORES + c
                arrived(None, rows_of(at), sem_tok.at[at])
                tokens_out.go(None, rows_of(at), rows_of(at), sem_tok.at[at], (me, partner))

        def take_tokens():
            for d in range(1, chips):
                at = (y + chips - d) % chips * CORES + (1 - c)
                arrived(None, rows_of(at), sem_tok.at[at])

        for h in range(1, last):
            spread_q.forward(h)
            if h > 1:
                project_p(h - 2, near)
            spread_kv.forward(h)
            if h == 1:
                spread_q.forward_next()
            project_q(h - 1, near)
            spread_p.forward(h)
            if h == 1:
                spread_kv.forward_next()
            project_kv(h - 1, near)
        spread_p.forward_side()
        spread_a.begin_down()
        spread_a.begin_up()
        spread_b.begin_down()
        spread_b.begin_up(at_end)
        gather_tokens()
        done = max(0, last - 1)
        if last:
            spread_q.forward(last)
        take_tokens()
        for h in range(done):
            project_q(h, far)
            project_kv(h, far)
        for h in range(max(0, last - 2)):
            project_p(h, far)
        if last:
            spread_kv.forward(last)
        for h in range(done, last):
            project_q(h, near + far)
            project_kv(h, near + far)
        if last:
            spread_p.forward(last)
        for h in range(max(0, last - 2), last):
            if h != 1:
                project_p(h, near + far)
        project_q(last, far + near)
        if last:
            project_p(1, far + near)
        project_kv(last, far + near)

        def settle(lo, hi):
            for chip in range(chips):
                r = slice(chip * per, (chip + 1) * per)
                ext[WINDOW + chip * per : WINDOW + (chip + 1) * per, lo:hi] = acc[r, lo:hi].astype(BF16)

        settle(0, channel0)

        halo_out, tot_out = [Sends(None), Sends(None)], Sends(tot)

        def pass_on(cond, at, width, n, i):
            head = ext.at[pl.ds(WINDOW - n, n), pl.ds(at, width)]
            tail = ext.at[pl.ds(seq + WINDOW - n, n), pl.ds(at, width)]
            halo_out[i].go(both(cond, later), tail, head, sem_halo.at[i], (me + 1, t))
            return head

        head_kv = pass_on(None, qw, kw + vw, WINDOW, 0)

        group = t * pw // POOL_CH
        whole_prefix = group == POOL_GROUPS - 1
        halos = [
            (group == g, -(-(reach - 1) // 16) * 16)
            for g, reach in enumerate(SHORT_REACHES + (WINDOW,))
        ]

        def finish_pool_rows(cond):
            def run():
                settle(channel0, ext.shape[1])
                for n in range(blocks):
                    r = slice(WINDOW + n * WINDOW, 2 * WINDOW + n * WINDOW)
                    total = jnp.sum(ext[r, channel0:].astype(F32), axis=0, keepdims=True)
                    if n + 1 < blocks:
                        carry[n + 1] = jnp.broadcast_to(
                            total if n == 0 else carry[n, 0:1, :] + total, carry.shape[1:]
                        )
                    else:
                        tot[me] = jnp.broadcast_to(
                            total if n == 0 else carry[n, 0:1, :] + total, tot.shape[1:]
                        )
                carry[0] = jnp.zeros(carry.shape[1:], F32)

            when(cond, run)
            for is_group, n in halos:
                pass_on(both(is_group, cond), channel0, pw, n, 1)
            for d in range(1, n_sp):
                tot_out.go(
                    both(both(whole_prefix, cond), me + d < n_sp), tot.at[me], tot.at[me],
                    sem_tot.at[0], (me + d, t),
                )

        finish_pool_rows(inner)
        spread_a.begin_x()
        spread_b.begin_x(inner)
        spread_b.begin_up(inner)
        if last:
            spread_a.forward(1, inner)

        group_heads = qw // kw
        stacked = group_heads * WINDOW
        scale = HEAD_DIM ** (-0.5)

        def attend(n):
            q_rows = pl.ds(pl.multiple_of(n * WINDOW + WINDOW, WINDOW), WINDOW)
            k_rows = pl.ds(pl.multiple_of(n * WINDOW, WINDOW), 2 * WINDOW)
            queries = ext[q_rows, :qw]
            keys = ext[k_rows, qw : qw + kw]
            values = ext[k_rows, qw + kw : channel0]
            row = lax.broadcasted_iota(jnp.int32, (stacked, 2 * WINDOW), 0)
            q_index = row % WINDOW
            k_index = lax.broadcasted_iota(jnp.int32, (stacked, 2 * WINDOW), 1)
            lowest = jnp.where(me * blocks + n == 0, WINDOW, 0)
            allowed = (k_index > q_index) & (k_index <= q_index + WINDOW) & (k_index >= lowest)
            which = lax.broadcasted_iota(jnp.int32, (stacked, 1), 0) // WINDOW
            done = []
            for j in range(kw // HEAD_DIM):
                part = slice(j * HEAD_DIM, (j + 1) * HEAD_DIM)
                first = j * group_heads
                q = jnp.concatenate(
                    [
                        queries[:, (first + g) * HEAD_DIM : (first + g + 1) * HEAD_DIM]
                        for g in range(group_heads)
                    ],
                    axis=0,
                )
                scores = (
                    lax.dot_general(
                        q, keys[:, part], (((1,), (1,)), ((), ())), preferred_element_type=F32
                    )
                    * scale
                )
                scores = jnp.where(allowed, scores, -jnp.inf)
                sinks = jnp.full((stacked, 1), sink[first], F32)
                for g in range(1, group_heads):
                    sinks = jnp.where(which == g, sink[first + g], sinks)
                peak = jnp.maximum(jnp.max(scores, axis=1, keepdims=True), sinks)
                expo = jnp.exp(scores - peak)
                denom = jnp.sum(expo, axis=1, keepdims=True) + jnp.exp(sinks - peak)
                probs = (expo * (1.0 / denom)).astype(BF16)
                got = jnp.dot(probs, values[:, part], preferred_element_type=F32)
                done += [got[g * WINDOW : (g + 1) * WINDOW] for g in range(group_heads)]
            to = pl.ds(pl.multiple_of(n * WINDOW, WINDOW), WINDOW)
            mix[to, :qw] = jnp.concatenate(done, axis=1).astype(BF16)

        if per % WINDOW == 0:
            span = per // WINDOW
            far_blocks, near_blocks = [chip * span for chip in far], [y * span]
        else:
            span = blocks
            far_blocks, near_blocks = [0], []

        def attend_later_blocks(firsts):
            for first in firsts:
                pl.loop(1, span, unroll=2 if span % 2 else 1)(lambda i, first=first: attend(first + i))

        def attend_first_block(firsts):
            for first in firsts:
                cond = earlier if isinstance(first, int) else both(earlier, first == 0)
                arrived(cond, head_kv, sem_halo.at[0])
                attend(first)

        reach = jnp.where(
            group == 0, SHORT_REACHES[0], jnp.where(group == 1, SHORT_REACHES[1], WINDOW)
        )
        reach = jnp.where(whole_prefix, n_sp * seq, reach)
        lowest = jnp.where(whole_prefix, WINDOW, 0)

        def pool(firsts):
            for first in firsts:

                @pl.loop(0, span)
                def _(i, first=first):
                    n = first + i
                    q_index = lax.broadcasted_iota(jnp.int32, (WINDOW, 2 * WINDOW), 0)
                    k_index = lax.broadcasted_iota(jnp.int32, (WINDOW, 2 * WINDOW), 1)
                    distance = q_index + WINDOW - k_index
                    band = (distance >= 0) & (distance < reach) & (k_index >= lowest)
                    band = jnp.where(band, 1.0, 0.0).astype(BF16)
                    k_rows = pl.ds(pl.multiple_of(n * WINDOW, WINDOW), 2 * WINDOW)
                    both_blocks = ext[k_rows, channel0:]
                    before = jnp.where(whole_prefix, carry[n, 0:1, :] + given[0:1, :], 0.0)
                    sums = jnp.dot(band, both_blocks, preferred_element_type=F32) + before
                    position = (
                        me * seq + n * WINDOW + lax.broadcasted_iota(jnp.int32, (WINDOW, 1), 0)
                    )
                    counted = jnp.minimum(position + 1, reach).astype(F32)
                    mixed = (sums / counted - both_blocks[WINDOW:].astype(F32)) * pgain[...]
                    to = pl.ds(pl.multiple_of(n * WINDOW, WINDOW), WINDOW)
                    mix[to, qw:] = mixed.astype(BF16)

        attend_later_blocks(far_blocks)
        if last >= 2:
            project_p(last, far + near)
        finish_pool_rows(at_end)
        spread_b.begin_x(at_end)
        if last:
            spread_a.forward(1, at_end)
            spread_b.forward(1, inner)
        attend_first_block(far_blocks)
        if last:
            spread_b.forward(1, at_end)
        spread_a.forward_next()
        for cond, n in halos:
            head = ext.at[pl.ds(WINDOW - n, n), pl.ds(channel0, pw)]
            arrived(both(cond, earlier), head, sem_halo.at[1])
        given[...] = jnp.zeros(given.shape, F32)
        for n in range(1, n_sp):

            def add(n=n):
                arrived(None, tot.at[pl.ds(0, n)], sem_tot.at[0])
                given[...] = jnp.sum(tot[:n], axis=0)

            when(both(whole_prefix, me == n), add)
        pool(far_blocks)

        def product(s, chip, core):
            r = pl.ds(pl.multiple_of((chip * CORES + core) * rows, rows), rows)
            return jnp.dot(mix[r, :qw], wa[s], preferred_element_type=F32) + jnp.dot(
                mix[r, qw:], wb[s], preferred_element_type=F32
            )

        far_out = Sends(dfar)
        near_out, y_out = Sends(dnear, late_sem.at[0]), Sends(ysend, late_sem.at[1])

        def multiply_far(pieces):
            for cond, s in pieces if chips > 1 else ():

                def give(s=s):
                    for i, chip in enumerate(far):
                        dfar[s, i] = product(s, chip, 1 - c).astype(BF16)

                def keep(s=s):
                    for i, chip in enumerate(far):
                        ofar[s, i] = product(s, chip, c)

                when(cond, give)
                far_out.go(cond, dfar.at[s], rfar.at[s], sem_far.at[s], (me, partner))
                when(cond, keep)

        def multiply_near(pieces):
            for cond, s in pieces:

                def give_near(s=s):
                    dnear[s] = product(s, y, 1 - c).astype(BF16)

                def keep_near(s=s):
                    onear[s] = product(s, y, c)

                when(cond, give_near)
                near_out.go(cond, dnear.at[s], rnear.at[s], sem_near.at[0], (me, partner))
                when(cond, keep_near)

        def finish(pieces):
            for cond, s in pieces if chips > 1 else ():

                def pack(s=s):
                    for i in range(chips - 1):
                        ysend[s, i] = (ofar[s, i] + rfar[s, i].astype(F32)).astype(BF16)

                arrived(cond, rfar.at[s], sem_far.at[s])
                when(cond, pack)
                for i, chip in enumerate(far):
                    y_out.go(
                        cond, ysend.at[s, i], yrecv.at[s, i], sem_y.at[s, i],
                        (me, chip * CORES + c),
                    )

        def multiply(pieces):
            for piece in pieces:
                multiply_far([piece])
                multiply_near([piece])
                finish([piece])

        first = column(0)
        second = column(1) if last else []
        third = others(0)
        multiply_far(first)
        multiply_far(second)
        finish(first)
        if last >= 2:
            spread_a.forward(2)
            spread_b.forward(2, inner)
        finish(second)
        attend_later_blocks(near_blocks)
        spread_b.forward_next()
        spread_a.take(0)
        spread_b.take(0)
        multiply_far(third)
        attend_first_block(near_blocks)
        finish(third)
        if last >= 2:
            spread_b.forward(2, at_end)
        spread_b.forward_side(z == last)
        spread_a.forward_side(z == last)
        fourth = column(2) if last >= 2 else []
        multiply_far(fourth)
        pool(near_blocks)
        multiply_near(first)
        finish(fourth)

        def only(cond, pieces):
            return [(both(there, cond), s) for there, s in pieces]


        def take_others(h, cond):
            spread_a.take(h, cond)
            spread_b.take(h, cond)
            multiply(only(cond, others(h)))

        if last > 1:
            take_others(1, at_end)
        if last >= 3:
            spread_a.forward(3)
        spread_b.forward_side(z == 0)
        spread_a.forward_side(z == 0)
        if last >= 3:
            spread_b.forward(3)
        left = second + third + fourth
        for h in range(3, last + 1):
            multiply_far(column(h))
            multiply_near(left[:2])
            finish(column(h))
            left = left[2:] + column(h)
        for h in range(2, last):
            spread_a.take(h)
            spread_b.take(h)
            multiply_far(others(h))
            multiply_near(left[:2])
            finish(others(h))
            left = left[2:] + others(h)
        multiply_near(left)
        if last > 1:
            take_others(1, inner)
        if last:
            take_others(last, None)

        for sends in groups:
            if sends is tokens_out:
                sends.wait_all()
            elif sends is far_out:
                sends.wait_all()
            else:
                sends.wait()
    dma = pltpu.SemaphoreType.DMA
    per_shard = dma((n_sp,))
    pl.run_scoped(
        gather_and_multiply, dma((n_in + n_out + 4,)), dma((SEND_GROUPS,)), per_shard, per_shard,
        per_shard, per_shard, per_shard, per_shard, dma((n_tp,)), dma((2,)), dma((1,)), per_shard,
    )

    order = column(0)
    if last:
        order = order + column(1)
    order = order + others(0)
    for h in range(2, last + 1):
        order = order + column(h)
    for h in range(1, last + 1):
        order = order + others(h)

    arrived(None, rnear, sem_near.at[0])
    w = wa.shape[2]
    for cond, s in order:

        def end(s=s):
            value = onear[s] + rnear[s].astype(F32)
            for i in range(chips - 1):
                arrived(None, yrecv.at[s, i], sem_y.at[s, i])
                value += yrecv[s, i].astype(F32)
            out[:, pl.ds(pl.multiple_of(s * w, w), w)] = value.astype(BF16)

        when(cond, end)

    for ref, i in ((dnear, 0), (ysend, 1)) if chips > 1 else ((dnear, 0),):
        pltpu.make_async_remote_copy(
            src_ref=ref, dst_ref=ref, send_sem=late_sem.at[i], recv_sem=sem_near.at[0],
            device_id=(me, partner), device_id_type=MESH,
        ).wait_send()


def kernel(n_sp, n_tp, cols, n_in, n_out, widths, *refs):
    dma = pltpu.SemaphoreType.DMA
    others = max(1, n_tp // CORES - 1)
    pl.run_scoped(
        functools.partial(layer, n_sp, n_tp, cols, n_in, n_out, widths, refs),
        dma((2,)), dma((1,)), dma((n_sp, others)),
    )


def local(
    n_sp, n_tp, tokens_in, norm_gain, query_weight, key_weight, value_weight, pool_weight,
    sink_logit, pool_gain, attention_out_weight, pool_out_weight,
):
    rows, depth = tokens_in.shape
    seq = rows * n_tp
    ins = [query_weight, key_weight, value_weight, pool_weight]
    outs = [attention_out_weight, pool_out_weight]
    widths = tuple(w.shape[1] for w in ins)
    if widths[1] % 128:
        ins = [ins[0], jnp.concatenate(ins[1:3], axis=1), ins[3]]
    cols = math.gcd(n_sp, max(1, n_tp // CORES))
    chips = n_tp // CORES
    k_in, out_cols = ins[0].shape[0], outs[0].shape[1]
    width, others = sum(widths), max(1, chips - 1)
    qw, kw, vw, pw = widths
    vmem = pl.BlockSpec(memory_space=pltpu.VMEM)
    hbm = pl.BlockSpec(memory_space=pl.ANY)
    return pl.pallas_call(
        functools.partial(kernel, n_sp, n_tp, cols, len(ins), len(outs), widths),
        out_shape=pltpu.VMEM((rows, depth), BF16),
        in_specs=[hbm] * (4 + len(ins) + len(outs)),
        out_specs=vmem,
        scratch_shapes=[
            pltpu.VMEM((rows, depth), BF16),
            pltpu.VMEM((n_sp, seq, depth // n_sp), BF16),
            pltpu.VMEM((n_sp, k_in, qw), BF16),
            pltpu.VMEM((n_sp, k_in, kw + vw), BF16),
            pltpu.VMEM((n_sp, k_in, pw), BF16),
            pltpu.VMEM((n_sp, outs[0].shape[0], out_cols), BF16),
            pltpu.VMEM((n_sp, outs[1].shape[0], out_cols), BF16),
            pltpu.VMEM((seq, width), F32),
            pltpu.VMEM((seq + WINDOW, width), BF16),
            pltpu.VMEM((seq, qw + pw), BF16),
            pltpu.VMEM((n_sp, 8, pw), F32),
            pltpu.VMEM((seq // WINDOW, 8, pw), F32),
            pltpu.VMEM((8, pw), F32),
            pltpu.VMEM((n_sp, others, rows, out_cols), BF16),
            pltpu.VMEM((n_sp, others, rows, out_cols), BF16),
            pltpu.VMEM((n_sp, rows, out_cols), BF16),
            pltpu.VMEM((n_sp, rows, out_cols), BF16),
            pltpu.VMEM((n_sp, others, rows, out_cols), BF16),
            pltpu.VMEM((n_sp, others, rows, out_cols), BF16),
            pltpu.VMEM((n_sp, others, rows, out_cols), F32),
            pltpu.VMEM((n_sp, rows, out_cols), F32),
            pltpu.VMEM((1, depth), F32),
            pltpu.VMEM((1, pw), F32),
            pltpu.SMEM(sink_logit.shape, F32),
        ],
        compiler_params=pltpu.CompilerParams(
            collective_id=0, has_side_effects=True, vmem_limit_bytes=58 << 20
        ),
    )(
        tokens_in, norm_gain.reshape(1, -1), sink_logit, pool_gain.reshape(1, -1), *ins, *outs
    )


def solution(mesh):
    in_specs = (
        P(("sp", "tp"), None), P(), P("sp", "tp"), P("sp", "tp"), P("sp", "tp"), P("sp", "tp"),
        P("tp"), P("tp"), P("tp", "sp"), P("tp", "sp"),
    )
    out_specs = P(("sp", "tp"), None)
    return jax.shard_map(
        functools.partial(local, mesh.shape["sp"], mesh.shape["tp"]),
        mesh=mesh, in_specs=in_specs, out_specs=out_specs, check_vma=False,
    )
```
